32 devices in a mesh: tp: 8 (over z, y), dp: 4 (over x, core).
Axes of the slice: x: 2, y: 2, z: 4, core: 2. Of those that a mesh axis runs over, the one named last changes fastest.
Arguments:
- stream: bfloat16 [128, 4096], P(None, ('dp', 'tp')), may hold values from -16 to 16
- lengths: int32 [128], P('dp'), may hold values from 1 to 64, 1024 in all
- prior_state: float32 [2, 128, 4096], P(None, 'dp', 'tp'), may hold values from -6 to 6
- prior_window: bfloat16 [2, 128, 3, 4096], P(None, 'dp', None, 'tp'), may hold values from -6 to 6
- norm_gain: float32 [2, 4096], P(None, 'dp'), may hold values from 0.1 to 1.9
- w_branch: bfloat16 [2, 4096, 4096], P(None, 'dp', 'tp'), may hold values from -0.09375 to 0.09375
- w_gate_branch: bfloat16 [2, 4096, 4096], P(None, 'dp', 'tp'), may hold values from -0.09375 to 0.09375
- conv_taps: bfloat16 [2, 4, 4096], P(None, None, 'tp'), may hold values from -3 to 3
- w_in_gate: bfloat16 [2, 256, 4096], P(None, None, 'tp'), may hold values from -0.375 to 0.375
- w_rec_gate: bfloat16 [2, 256, 4096], P(None, None, 'tp'), may hold values from -0.375 to 0.375
- decay_param: float32 [2, 4096], P(None, 'tp'), may hold values from -1 to 4
- w_out: bfloat16 [2, 4096, 4096], P(None, 'tp', 'dp'), may hold values from -0.1875 to 0.1875
Outputs:
- mixed_out: bfloat16 [128, 4096], P(None, ('dp', 'tp'))
- new_state: float32 [2, 128, 4096], P(None, 'dp', 'tp')
- new_window: bfloat16 [2, 128, 3, 4096], P(None, 'dp', None, 'tp')
The draws below stay inside these ranges and needn't reach their ends.
All inputs are finite; a program needn't handle non-finite values. No bound on the sum of `lengths` on one device may be relied on, other than what follows from the above.
Results may differ from the reference program's by a relative error of at most 0.014.
Values may be sent and summed in bfloat16 or wider, within the bound.
A program may use at most 64 MiB of HBM per device.

```python
import math
import jax
import jax.numpy as jnp
import numpy as np
from jax import lax

D = 4096
D_RNN = 4096
BLOCK = 256
TAPS = 4
LAYERS = 2
BATCH = 128
N_TP = 8
N_DP = 4


def draw_stream(key, part):
    feature = jnp.arange(D)
    per_device = D // (N_DP * N_TP)
    along_dp = (feature // (D // N_DP)).astype(jnp.float32) / max(N_DP - 1, 1)
    along_tp = (feature // per_device % N_TP).astype(jnp.float32) / max(N_TP - 1, 1)
    rising = jnp.exp(jnp.log(3.0) * (along_dp + along_tp))
    values = jax.random.normal(key, (BATCH, D), jnp.float32) * 0.4 * rising
    return jnp.clip(values, -16.0, 16.0).astype(jnp.bfloat16)


def strengthened(values, stream_key, source, target, shards_of, factor):
    def block_of(axis_at):
        return (jnp.arange(values.shape[axis_at]) // (values.shape[axis_at] // shards_of)).reshape((-1,) + (1,) * (values.ndim - 1 - axis_at))

    near = jax.random.permutation(stream_key, shards_of)[block_of(target)]
    far = (block_of(target) + shards_of // 2) % shards_of
    return jnp.where((block_of(source) == near) | (block_of(source) == far), factor * values, values)


def levels(own_key, dims, split, least, largest):
    def one(axis_at, shards_of):
        draws = jax.random.uniform(jax.random.fold_in(jax.random.fold_in(own_key, 6), axis_at), (shards_of,), jnp.float32, least / len(split), largest / len(split))
        return jnp.repeat(jnp.exp(draws), dims[axis_at] // shards_of).reshape((-1,) + (1,) * (len(dims) - axis_at - 1))

    loudness = one(*split[0])
    for cut in split[1:]:
        loudness = loudness * one(*cut)
    return loudness


def split_up(amount, total, most, lean):
    portions = [(1 << 20) // math.isqrt(standing ** lean) + 1 for standing in range(2, amount + 1)]
    surplus, holding = total - most - (amount - 1), [1] * (amount - 1)
    while surplus > 0:
        candidates = [i for i in range(amount - 1) if holding[i] < most]
        whole, left = sum([portions[i] for i in candidates]), surplus
        for i in candidates:
            addition = min(most - holding[i], max(1, left * portions[i] // whole), surplus)
            holding[i] = holding[i] + addition
            surplus = surplus - addition
    return np.array([most] + holding)


def ragged_sizes(key, count, total, reach, skew):
    if count == 2:
        one = jax.random.randint(key, (), max(1, total - reach), min(reach, total - 1) + 1)
        return jnp.stack([one, total - one])
    sizes = jnp.asarray(split_up(count, total, reach, skew), jnp.int32)
    twos = (count - 1) // 2
    giver, receiver = sizes[1:1 + 2 * twos:2], sizes[2:2 + 2 * twos:2]
    margin = jnp.minimum(giver - 1, reach - receiver)
    moved = jax.random.randint(jax.random.fold_in(key, 1), (twos,), 0, 1 << 20) % (margin + 1)
    sizes = sizes.at[1:1 + 2 * twos:2].set(giver - moved).at[2:2 + 2 * twos:2].set(receiver + moved)
    return sizes[jax.random.permutation(jax.random.fold_in(key, 2), count)]


def gaussian(stream_key, shape, deviation, reach, split=(), held_as=jnp.bfloat16):
    array = deviation * jax.random.normal(stream_key, shape, jnp.float32)
    if split:
        array = array * levels(stream_key, shape, split, -0.22, 0.18)
    return jnp.clip(array, -reach, reach).astype(held_as)


def heavy_noise(stream_key, extent, deviation, most, split, heavy, kind=jnp.bfloat16):
    values = deviation * jax.random.normal(stream_key, extent, jnp.float32)
    if split:
        values = values * levels(stream_key, extent, split, -0.22, 0.18)
    return jnp.clip(strengthened(values, jax.random.fold_in(stream_key, 3), *heavy), -most, most).astype(kind)


def setup_inputs(seed: int = 0) -> dict:
    arg_keys = jax.random.split(jax.random.key(seed), 13)
    stream = draw_stream(jax.random.fold_in(arg_keys[12], 71), 0)
    lengths = ragged_sizes(arg_keys[1], BATCH, 8 * BATCH, 64, 2).astype(jnp.int32)
    prior_state = gaussian(arg_keys[2], (LAYERS, BATCH, D_RNN), 1.0, 6.0, ((1, 4), (2, 8)), jnp.float32)
    prior_window = gaussian(arg_keys[3], (LAYERS, BATCH, TAPS - 1, D_RNN), 1.0, 6.0, ((1, 4), (3, 8)))
    norm_gain = jnp.clip(1.0 + 0.18 * jax.random.normal(arg_keys[4], (LAYERS, D), jnp.float32), 0.1, 1.9)
    w_branch = gaussian(arg_keys[5], (LAYERS, D, D_RNN), D ** -0.5, 0.09375, ((1, 4), (2, 8)))
    w_gate_branch = gaussian(arg_keys[6], (LAYERS, D, D_RNN), D ** -0.5, 0.09375, ((1, 4), (2, 8)))
    conv_taps = gaussian(arg_keys[7], (LAYERS, TAPS, D_RNN), TAPS ** -0.5, 3.0, ((2, 8),))
    w_in_gate = gaussian(arg_keys[8], (LAYERS, BLOCK, D_RNN), BLOCK ** -0.5, 0.375, ((2, 8),))
    w_rec_gate = gaussian(arg_keys[9], (LAYERS, BLOCK, D_RNN), BLOCK ** -0.5, 0.375, ((2, 8),))
    decay_param = jnp.clip(-1.0 + 5.0 * jax.random.uniform(arg_keys[10], (LAYERS, D_RNN), jnp.float32) ** levels(arg_keys[10], (LAYERS, D_RNN), ((1, 8),), -0.2, 0.2), -1.0, 4.0)
    w_out = heavy_noise(arg_keys[11], (LAYERS, D_RNN, D), (D_RNN // 2) ** -0.5, 0.1875, ((1, 8), (2, 4)), (1, 2, 8, 2.0))
    return {"stream": stream, "lengths": lengths, "prior_state": prior_state, "prior_window": prior_window, "norm_gain": norm_gain, "w_branch": w_branch, "w_gate_branch": w_gate_branch, "conv_taps": conv_taps, "w_in_gate": w_in_gate, "w_rec_gate": w_rec_gate, "decay_param": decay_param, "w_out": w_out}


epsilon = 1e-06

def block_map(convolved, weight):
    row_count = convolved.shape[0]
    blocks = D_RNN // BLOCK
    inputs = convolved.astype(jnp.float32).reshape(row_count, blocks, BLOCK)
    tables = weight.astype(jnp.float32).reshape(BLOCK, blocks, BLOCK)
    return jnp.einsum('rnk,knc->rnc', inputs, tables).reshape(row_count, D_RNN)

def projected(normed, weight):
    block_width = D // N_DP

    def add_block(running, index):
        offset = (index * block_width).astype(jnp.int32)
        columns = lax.dynamic_slice_in_dim(normed, offset, block_width, 1)
        weight_rows = lax.dynamic_slice_in_dim(weight, offset, block_width, 0)
        partial_sum = jnp.dot(columns, weight_rows, preferred_element_type=jnp.float32).astype(jnp.bfloat16)
        partial_sum = lax.optimization_barrier(partial_sum)
        return (running + partial_sum.astype(jnp.float32), None)
    start_sum = jnp.zeros((normed.shape[0], weight.shape[1]), jnp.float32)
    running, _ = lax.scan(add_block, start_sum, jnp.arange(N_DP, dtype=jnp.int32))
    return running.astype(jnp.bfloat16)

def recurrent_block(stream, lengths, prior_state, prior_window, norm_gain, w_branch, w_gate_branch, conv_taps, w_in_gate, w_rec_gate, decay_param, w_out):
    widened = stream.astype(jnp.float32)
    squares = lax.optimization_barrier(jnp.sum(widened * widened, axis=1, keepdims=True))
    normed = (widened * lax.rsqrt(squares / D + epsilon) * norm_gain).astype(jnp.bfloat16)
    branch = projected(normed, w_branch)
    gate_in = projected(normed, w_gate_branch)
    depth = prior_window.shape[1]
    needed = depth + 1 - jnp.arange(depth, dtype=jnp.int32)
    living = lengths[:, None, None] >= needed[None, :, None]
    history = jnp.where(living, prior_window, jnp.zeros_like(prior_window))
    window = jnp.concatenate([history, branch[:, None, :]], axis=1)
    convolved = lax.optimization_barrier(jnp.sum(window.astype(jnp.float32) * conv_taps.astype(jnp.float32)[None], axis=1)).astype(jnp.bfloat16)
    input_gate = jax.nn.sigmoid(block_map(convolved, w_in_gate))
    recur_gate = jax.nn.sigmoid(block_map(convolved, w_rec_gate))
    log_keep = 8.0 * recur_gate * jax.nn.log_sigmoid(decay_param)
    keeping = jnp.exp(log_keep)
    feeding = jnp.sqrt(-jnp.expm1(2.0 * log_keep))
    earlier = jnp.where(lengths[:, None] >= 2, prior_state, jnp.zeros_like(prior_state))
    state = keeping * earlier + feeding * input_gate * convolved.astype(jnp.float32)
    readout = (state * jax.nn.gelu(gate_in.astype(jnp.float32))).astype(jnp.bfloat16)
    result = (widened + jnp.dot(readout, w_out, preferred_element_type=jnp.float32)).astype(jnp.bfloat16)
    return (result, state, window[:, 1:])

def reference(stream, lengths, prior_state, prior_window, norm_gain, w_branch, w_gate_branch, conv_taps, w_in_gate, w_rec_gate, decay_param, w_out):
    first, state_first, window_first = recurrent_block(stream, lengths, prior_state[0], prior_window[0], norm_gain[0], w_branch[0], w_gate_branch[0], conv_taps[0], w_in_gate[0], w_rec_gate[0], decay_param[0], w_out[0])
    second, state_second, window_second = recurrent_block(first, lengths, prior_state[1], prior_window[1], norm_gain[1], w_branch[1], w_gate_branch[1], conv_taps[1], w_in_gate[1], w_rec_gate[1], decay_param[1], w_out[1])
    return (second, jnp.stack([state_first, state_second]), jnp.stack([window_first, window_second]))
```

```python
import functools

import jax
import jax.numpy as jnp
from jax import lax
from jax.experimental import pallas as pl
from jax.experimental.pallas import tpu as pltpu
from jax.sharding import PartitionSpec as P

D = 4096
BLOCK = 256


epsilon = 1e-06


def from_partner(block, axis, apart):
    count = lax.axis_size(axis)
    route = []
    for low in range(count):
        high = low | 1 << apart
        if high != low and high < count:
            route += [(low, high), (high, low)]
    return lax.ppermute(block, axis, route)


def norm_rows(block_rows, gain_values, squares):
    scaling = lax.rsqrt(squares / D + epsilon)
    return (block_rows.astype(jnp.float32) * scaling * gain_values).astype(jnp.bfloat16)


def normed_input(stream_local, gain_block):
    own_width = stream_local.shape[1]
    offset = lax.axis_index("tp") * own_width
    widened = stream_local.astype(jnp.float32)
    squares = lax.psum(jnp.sum(widened * widened, axis=1, keepdims=True), ("tp", "dp"))
    own_gain = lax.dynamic_slice_in_dim(gain_block, offset, own_width, 0)
    result = lax.all_gather(norm_rows(stream_local, own_gain, squares), "tp", axis=1, tiled=True)
    return result


def peer_block(convolved):
    col_count = convolved.shape[1]
    group_size = max(BLOCK // col_count, 1)
    device = lax.axis_index("tp")
    grouped = convolved
    for bit_number in range(group_size.bit_length() - 1):
        partner = from_partner(grouped, "tp", bit_number)
        is_upper = device // (1 << bit_number) % 2 == 1
        grouped = jnp.where(
            is_upper,
            jnp.concatenate([partner, grouped], axis=1),
            jnp.concatenate([grouped, partner], axis=1),
        )
    return grouped


def block_gates(grouped, weight):
    row_count = grouped.shape[0]
    col_count = weight.shape[1]
    blocks = max(col_count // BLOCK, 1)
    block_cols = min(col_count, BLOCK)
    inputs = grouped.reshape(row_count, blocks, BLOCK)
    tables = weight.reshape(BLOCK, blocks, block_cols)
    mapped = jnp.einsum("rnk,knc->rnc", inputs, tables, preferred_element_type=jnp.float32)
    return mapped.reshape(row_count, col_count)


def recurrent_step(
    normed,
    lengths,
    prior_state,
    prior_window,
    w_branch,
    w_gate_branch,
    conv_taps,
    w_in_gate,
    w_rec_gate,
    decay_param,
    w_out,
    stream_local,
):
    col_count = w_branch.shape[1]
    summed = lax.psum_scatter(
        jnp.concatenate(
            [
                jnp.dot(normed, w_branch, preferred_element_type=jnp.float32),
                jnp.dot(normed, w_gate_branch, preferred_element_type=jnp.float32),
            ],
            axis=1,
        ).astype(jnp.bfloat16),
        "dp",
        scatter_dimension=0,
        tiled=True,
    ).astype(jnp.float32)
    branch = summed[:, :col_count].astype(jnp.bfloat16)
    gate_in = summed[:, col_count:].astype(jnp.bfloat16)
    depth = prior_window.shape[1]
    needed = depth + 1 - jnp.arange(depth, dtype=jnp.int32)
    living = lengths[:, None, None] >= needed[None, :, None]
    history = jnp.where(living, prior_window, jnp.zeros_like(prior_window))
    window = jnp.concatenate([history, branch[:, None, :]], axis=1)
    convolved = jnp.sum(
        window.astype(jnp.float32) * conv_taps.astype(jnp.float32)[None], axis=1
    ).astype(jnp.bfloat16)
    grouped = peer_block(convolved)
    input_gate = jax.nn.sigmoid(block_gates(grouped, w_in_gate))
    recur_gate = jax.nn.sigmoid(block_gates(grouped, w_rec_gate))
    log_keep = 8.0 * recur_gate * jax.nn.log_sigmoid(decay_param)
    keeping = jnp.exp(log_keep)
    feeding = jnp.sqrt(-jnp.expm1(2.0 * log_keep))
    earlier = jnp.where(lengths[:, None] >= 2, prior_state, jnp.zeros_like(prior_state))
    state = keeping * earlier + feeding * input_gate * convolved.astype(jnp.float32)
    readout = (state * jax.nn.gelu(gate_in.astype(jnp.float32))).astype(jnp.bfloat16)
    mixed = jnp.dot(
        lax.all_gather(readout, "dp", axis=0, tiled=True), w_out, preferred_element_type=jnp.float32
    )
    own_width = stream_local.shape[1]
    offset = lax.axis_index("tp") * own_width
    own_cols = lax.dynamic_slice_in_dim(mixed, offset, own_width, 1) + stream_local.astype(
        jnp.float32
    )
    terms = lax.dynamic_update_slice_in_dim(mixed, own_cols, offset, 1)
    return (terms, state, window[:, 1:])


def body(
    stream,
    lengths,
    prior_state,
    prior_window,
    norm_gain,
    w_branch,
    w_gate_branch,
    conv_taps,
    w_in_gate,
    w_rec_gate,
    decay_param,
    w_out,
):
    normed = normed_input(stream, norm_gain[0])
    terms, state_first, window_first = recurrent_step(
        normed,
        lengths,
        prior_state[0],
        prior_window[0],
        w_branch[0],
        w_gate_branch[0],
        conv_taps[0],
        w_in_gate[0],
        w_rec_gate[0],
        decay_param[0],
        w_out[0],
        stream,
    )
    carried = lax.psum(terms, "tp").astype(jnp.bfloat16)
    widened = carried.astype(jnp.float32)
    squares = lax.psum(jnp.sum(widened * widened, axis=1, keepdims=True), "dp")
    normed = norm_rows(carried, norm_gain[1], squares)
    own_width = stream.shape[1]
    first = lax.dynamic_slice_in_dim(carried, lax.axis_index("tp") * own_width, own_width, 1)
    terms, state_second, window_second = recurrent_step(
        normed,
        lengths,
        prior_state[1],
        prior_window[1],
        w_branch[1],
        w_gate_branch[1],
        conv_taps[1],
        w_in_gate[1],
        w_rec_gate[1],
        decay_param[1],
        w_out[1],
        first,
    )
    second = lax.psum_scatter(terms, "tp", scatter_dimension=1, tiled=True).astype(jnp.bfloat16)
    return (
        second,
        jnp.stack([state_first, state_second]),
        jnp.stack([window_first, window_second]),
    )


HALVES = 4
MAIN_VMEM = 60 * 1024 * 1024
TAIL_VMEM = 4 * 1024 * 1024
MESH = pl.DeviceIdType.MESH


def negative_expm1(z):
    series = -z * (1.0 + z / 2.0 * (1.0 + z / 3.0 * (1.0 + z / 4.0 * (1.0 + z / 5.0))))
    return jnp.where(z > -0.1, series, 1.0 - jnp.exp(z))


def fused_kernel(
    nt,
    nd,
    halves,
    stream,
    lengths,
    prior_state,
    prior_window,
    norm_gain,
    w_branch,
    w_gate_branch,
    conv_taps,
    w_in_gate,
    w_rec_gate,
    decay_param,
    w_out,
    mix_o,
    state_o,
    hist_o,
    branch_o,
    xg,
    part,
    pr,
    half,
    px,
    ro,
    rg,
    mx,
    ms,
    aux,
    len_v,
    state_v,
    win_v,
    gain_v,
    wp_v,
    taps_v,
    gates_v,
    decay_v,
    wo_v,
    in_sem,
    sent,
    xr,
    pr_r,
    px_r,
    gr,
    ms_r,
    as_r,
):
    t = lax.axis_index("tp")
    d = lax.axis_index("dp")
    side = d // 2
    mate = d + 1 - 2 * lax.rem(d, 2)
    across = lax.rem(d + 2, nd)
    layers = w_branch.shape[0]
    rows, own = stream.shape[1], stream.shape[2]
    r = rows // halves
    cols = w_branch.shape[2]
    width = w_branch.shape[1]
    depth = prior_window.shape[1]

    barrier = pltpu.get_barrier_semaphore()
    tp_peers = [(k, flipped(t, k, nt)) for k in range(nt - 1, 0, -1)]
    for _, peer in tp_peers:
        pl.semaphore_signal(barrier, inc=1, device_id={"tp": peer}, device_id_type=MESH)
    for peer in (across, mate):
        pl.semaphore_signal(barrier, inc=1, device_id={"dp": peer}, device_id_type=MESH)

    counter = [0]

    def load(*pairs):
        sem = in_sem.at[counter[0]]
        counter[0] += 1
        for src, dst in pairs:
            pltpu.make_async_copy(src, dst, sem).start()
        return sem

    def loaded(ref, sem):
        pltpu.make_async_copy(ref, ref, sem).wait()

    c_stream = load(*[(stream.at[block_of(d, s)], xg.at[0, t, s]) for s in range(nd)])
    c_first = [
        (held, load((src, held)))
        for src, held in (
            (lengths, len_v),
            (conv_taps, taps_v),
            (prior_window, win_v),
            (prior_state, state_v),
        )
    ]
    c_gain = load((norm_gain, gain_v))
    c_w, c_o = [], []
    for l in range(layers):
        c_w.append(load((w_branch.at[l], wp_v.at[l, 0]), (w_gate_branch.at[l], wp_v.at[l, 1])))
        if l == 0:
            c_gates = load((w_in_gate, gates_v.at[0]), (w_rec_gate, gates_v.at[1]))
            c_decay = load((decay_param, decay_v))
        c_o.append(load((w_out.at[l], wo_v.at[l])))

    def remote(src, dst, ssem, rsem, axis, peer):
        return pltpu.make_async_remote_copy(
            src_ref=src,
            dst_ref=dst,
            send_sem=ssem,
            recv_sem=rsem,
            device_id={axis: peer},
            device_id_type=MESH,
        )

    def send(src, dst, kind, rsem, axis, peer):
        remote(src, dst, sent.at[kind], rsem, axis, peer).start()

    def arrived(ref, rsem, axis, peer):
        remote(ref, ref, sent.at[0], rsem, axis, peer).wait_recv()

    def all_sent(ref, kind, axis, peer):
        remote(ref, ref, sent.at[kind], sent.at[kind], axis, peer).wait_send()

    def cut(h):
        return slice(h * r, (h + 1) * r)

    def send_features(l, h):
        block = xg.at[l, t, :, pl.ds(h * r, r), :]
        for _, peer in tp_peers:
            send(block, block, 0, xr.at[l, h], "tp", peer)

    def prepare():
        length = jnp.sum(
            jnp.where(
                lax.broadcasted_iota(jnp.int32, (rows, rows), 0)
                == lax.broadcasted_iota(jnp.int32, (rows, rows), 1),
                jnp.broadcast_to(len_v[...].astype(jnp.float32), (rows, rows)),
                0.0,
            ),
            axis=1,
            keepdims=True,
        )
        for l in range(layers):
            taps = taps_v[l].astype(jnp.float32)
            before = jnp.zeros((rows, cols), jnp.float32)
            for m in range(depth):
                row = win_v[l, m].astype(jnp.float32)
                row = jnp.where(length >= depth + 1 - m, row, 0.0)
                before = before + row * taps[m : m + 1]
                if m > 0:
                    hist_o[l, m - 1] = row.astype(jnp.bfloat16)
            aux[l, side, 0] = before
            aux[l, side, 1] = jnp.where(length >= 2, state_v[l], 0.0)

    def send_history(l):
        block = aux.at[l, side]
        send(block, block, 5, as_r.at[l], "dp", across)

    def project(l, h):
        arrived(xg.at[l, pl.ds(0, nt - 1), :, pl.ds(h * r, r), :], xr.at[l, h], "tp", tp_peers[0][1])
        if h == 0:
            if l == 0:
                loaded(gain_v, c_gain)
            loaded(wp_v.at[l], c_w[l])
        squares = jnp.zeros((nd * r, own), jnp.float32)
        pieces = []
        for j in range(nt):
            x = xg[l, j, :, cut(h), :].reshape(nd * r, own).astype(jnp.float32)
            squares = squares + x * x
            gain = gain_v[l : l + 1, j * own : (j + 1) * own]
            pieces.append((x * gain).astype(jnp.bfloat16))
        normed = jnp.concatenate(pieces, axis=1)
        total = jnp.sum(squares, axis=1, keepdims=True)
        high = total.astype(jnp.bfloat16).astype(jnp.float32)
        lane = lax.broadcasted_iota(jnp.int32, (nd * r, 128), 1)
        both = jnp.where(lane < 64, high, total - high).astype(jnp.bfloat16)
        part[l, h, :, :, 2 * cols :] = both.reshape(nd, r, 128)
        for w in range(2):
            product = jnp.dot(normed, wp_v[l, w], preferred_element_type=jnp.float32)
            part[l, h, :, :, w * cols : (w + 1) * cols] = product.astype(jnp.bfloat16).reshape(
                nd, r, cols
            )
        send(part.at[l, h, pl.ds(2, 2)], pr.at[l, h], 1, pr_r.at[l, h], "dp", mate)

    def halve(l, h):
        arrived(pr.at[l, h], pr_r.at[l, h], "dp", mate)
        both = part[l, h, 0:2].astype(jnp.float32) + pr[l, h].astype(jnp.float32)
        half[l, h] = both.astype(jnp.bfloat16)
        send(half.at[l, h], px.at[l, h], 2, px_r.at[l, h], "dp", across)

    def recur(l, h):
        if h == 0:
            if l == 0:
                loaded(gates_v, c_gates)
                loaded(decay_v, c_decay)
            arrived(aux.at[l, 1 - side], as_r.at[l], "dp", across)
        before = aux[l, :, 0, cut(h), :].reshape(2 * r, cols)
        earlier = aux[l, :, 1, cut(h), :].reshape(2 * r, cols)
        taps = taps_v[l].astype(jnp.float32)
        raw = decay_v[l : l + 1]
        log_decay = jnp.minimum(raw, 0.0) - jnp.log1p(jnp.exp(-jnp.abs(raw)))

        arrived(px.at[l, h], px_r.at[l, h], "dp", across)
        summed = half[l, h].astype(jnp.float32) + px[l, h].astype(jnp.float32)
        summed = summed.reshape(2 * r, 2 * cols + 128)
        squares = summed[:, 2 * cols : 2 * cols + 1] + summed[:, 2 * cols + 64 : 2 * cols + 65]
        scaling = lax.rsqrt(squares / (width * nd) + epsilon)
        branch = (summed[:, :cols] * scaling).astype(jnp.bfloat16)
        gate_in = (summed[:, cols : 2 * cols] * scaling).astype(jnp.bfloat16)
        branch_o[l, :, cut(h), :] = branch.reshape(2, r, cols)
        convolved = (before + branch.astype(jnp.float32) * taps[depth : depth + 1]).astype(
            jnp.bfloat16
        )
        mapped = []
        for w in range(2):
            mapped.append(
                jnp.concatenate(
                    [
                        jnp.dot(
                            convolved[:, n * BLOCK : (n + 1) * BLOCK],
                            gates_v[w, l, :, n * BLOCK : (n + 1) * BLOCK],
                            preferred_element_type=jnp.float32,
                        )
                        for n in range(cols // BLOCK)
                    ],
                    axis=1,
                )
            )
        input_gate = jax.nn.sigmoid(mapped[0])
        recur_gate = jax.nn.sigmoid(mapped[1])
        log_keep = 8.0 * recur_gate * log_decay
        feeding = jnp.sqrt(negative_expm1(2.0 * log_keep))
        state = jnp.exp(log_keep) * earlier + feeding * input_gate * convolved.astype(jnp.float32)
        state_o[l, :, cut(h), :] = state.reshape(2, r, cols)
        readout = (state * jax.nn.gelu(gate_in.astype(jnp.float32))).astype(jnp.bfloat16)
        ro[l, h] = readout.reshape(2, r, cols)
        send(ro.at[l, h], rg.at[l, h], 3, gr.at[l, h], "dp", mate)

    def mix(l, h):
        if h == 0:
            loaded(wo_v.at[l], c_o[l])
        arrived(rg.at[l, h], gr.at[l, h], "dp", mate)
        readout = jnp.concatenate(
            [ro[l, h].reshape(2 * r, cols), rg[l, h].reshape(2 * r, cols)], axis=0
        )
        mixed = jnp.dot(readout, wo_v[l], preferred_element_type=jnp.float32)
        for j in range(nt):
            mx[l, h, j] = mixed[:, j * own : (j + 1) * own].astype(jnp.bfloat16)
        for k, peer in tp_peers:
            send(mx.at[l, h, peer], ms.at[l, h, k - 1], 4, ms_r.at[l, h], "tp", peer)

    def collect(l, h):
        total = mx[l, h, t].astype(jnp.float32)
        total = total + xg[l, t, :, cut(h), :].reshape(nd * r, own).astype(jnp.float32)
        arrived(ms.at[l, h], ms_r.at[l, h], "tp", tp_peers[0][1])
        for k in range(nt - 1):
            total = total + ms[l, h, k].astype(jnp.float32)
        result = total.astype(jnp.bfloat16).reshape(nd, r, own)
        if l + 1 < layers:
            xg[l + 1, t, :, cut(h), :] = result
            send_features(l + 1, h)
        else:
            mix_o[:, cut(h), :] = result

    loaded(xg.at[0, t], c_stream)
    pl.semaphore_wait(barrier, nt - 1 + 2)
    for h in range(halves):
        send_features(0, h)
    for ref, sem in c_first:
        loaded(ref, sem)
    prepare()
    send_history(0)
    for l in range(layers):
        for h in range(halves):
            project(l, h)
            if h > 0:
                halve(l, h - 1)
        halve(l, halves - 1)
        for h in range(halves):
            recur(l, h)
            if h > 0:
                mix(l, h - 1)
        mix(l, halves - 1)
        if l + 1 < layers:
            send_history(l + 1)
        for h in range(halves):
            collect(l, h)
    all_sent(xg.at[:, pl.ds(0, nt - 1)], 0, "tp", tp_peers[0][1])
    all_sent(pr, 1, "dp", mate)
    all_sent(px, 2, "dp", across)
    all_sent(rg, 3, "dp", mate)
    all_sent(ms, 4, "tp", tp_peers[0][1])
    all_sent(aux.at[:, 0], 5, "dp", across)


def flipped(index, mask, count):
    for bit in range(count.bit_length() - 1):
        if mask >> bit & 1:
            index = index + (1 << bit) * (1 - 2 * (index // (1 << bit) % 2))
    return index


def block_of(d, s):
    core = lax.rem(d, 2)
    return 2 * (s % 2) + (core if s < 2 else 1 - core)


def tail_kernel(mixed, state, hist, branch, mixed_out, state_out, window_out, sem):
    d = lax.axis_index("dp")
    side = d // 2
    layers, depth = window_out.shape[:2]
    pairs = [(mixed.at[s], mixed_out.at[block_of(d, s)]) for s in range(mixed.shape[0])]
    for l in range(layers):
        pairs.append((state.at[l, side], state_out.at[l]))
        pairs.append((hist.at[l], window_out.at[l, pl.ds(0, depth - 1)]))
        pairs.append((branch.at[l, side], window_out.at[l, depth - 1]))
    stores = [pltpu.make_async_copy(src, dst, sem.at[k]) for k, (src, dst) in enumerate(pairs)]
    for copy in stores:
        copy.start()
    for copy in stores:
        copy.wait()


def fused(
    nt,
    nd,
    halves,
    stream,
    lengths,
    prior_state,
    prior_window,
    norm_gain,
    w_branch,
    w_gate_branch,
    conv_taps,
    w_in_gate,
    w_rec_gate,
    decay_param,
    w_out,
):
    layers, width, cols = w_branch.shape
    batch, own = stream.shape
    rows = batch // nd
    r = rows // halves
    depth = prior_window.shape[2]
    window = prior_window.transpose(0, 2, 1, 3)
    bf16, f32 = jnp.bfloat16, jnp.float32
    anywhere = pl.BlockSpec(memory_space=pl.ANY)
    held = pl.BlockSpec(memory_space=pltpu.VMEM)
    dma = pltpu.SemaphoreType.DMA
    finals = pl.pallas_call(
        functools.partial(fused_kernel, nt, nd, halves),
        out_shape=(
            pltpu.VMEM((nd, rows, own), bf16),
            pltpu.VMEM((layers, 2, rows, cols), f32),
            pltpu.VMEM((layers, depth - 1, rows, cols), bf16),
            pltpu.VMEM((layers, 2, rows, cols), bf16),
        ),
        in_specs=[pl.BlockSpec(memory_space=pltpu.HBM)] * 12,
        out_specs=(held,) * 4,
        scratch_shapes=[
            pltpu.VMEM((layers, nt, nd, rows, own), bf16),
            pltpu.VMEM((layers, halves, nd, r, 2 * cols + 128), bf16),
            pltpu.VMEM((layers, halves, 2, r, 2 * cols + 128), bf16),
            pltpu.VMEM((layers, halves, 2, r, 2 * cols + 128), bf16),
            pltpu.VMEM((layers, halves, 2, r, 2 * cols + 128), bf16),
            pltpu.VMEM((layers, halves, 2, r, cols), bf16),
            pltpu.VMEM((layers, halves, 2, r, cols), bf16),
            pltpu.VMEM((layers, halves, nt, nd * r, own), bf16),
            pltpu.VMEM((layers, halves, nt - 1, nd * r, own), bf16),
            pltpu.VMEM((layers, 2, 2, rows, cols), f32),
            pltpu.VMEM((1, rows), jnp.int32),
            pltpu.VMEM(prior_state.shape, f32),
            pltpu.VMEM(window.shape, bf16),
            pltpu.VMEM(norm_gain.shape, f32),
            pltpu.VMEM((layers, 2, width, cols), bf16),
            pltpu.VMEM(conv_taps.shape, bf16),
            pltpu.VMEM((2, layers, BLOCK, cols), bf16),
            pltpu.VMEM(decay_param.shape, f32),
            pltpu.VMEM(w_out.shape, bf16),
            dma((8 + 2 * layers,)),
            dma((6,)),
            dma((layers, halves)),
            dma((layers, halves)),
            dma((layers, halves)),
            dma((layers, halves)),
            dma((layers, halves)),
            dma((layers,)),
        ],
        compiler_params=pltpu.CompilerParams(
            collective_id=0, has_side_effects=True, vmem_limit_bytes=MAIN_VMEM
        ),
    )(
        stream.reshape(nd, rows, own),
        lengths.reshape(1, rows),
        prior_state,
        window,
        norm_gain,
        w_branch,
        w_gate_branch,
        conv_taps,
        w_in_gate,
        w_rec_gate,
        decay_param,
        w_out,
    )
    mixed, state, new_window = pl.pallas_call(
        tail_kernel,
        out_shape=(
            jax.ShapeDtypeStruct((nd, rows, own), bf16),
            jax.ShapeDtypeStruct(prior_state.shape, f32),
            jax.ShapeDtypeStruct(window.shape, bf16),
        ),
        in_specs=[held] * 4,
        out_specs=(anywhere,) * 3,
        scratch_shapes=[dma((nd + 3 * layers,))],
        compiler_params=pltpu.CompilerParams(vmem_limit_bytes=TAIL_VMEM),
    )(*finals)
    return mixed.reshape(batch, own), state, new_window.transpose(0, 2, 1, 3)


def step(nt, nd, *arrays):
    stream, w_branch = arrays[0], arrays[5]
    rows, cols = stream.shape[0] // nd, w_branch.shape[2]
    if nd == 4 and nt & (nt - 1) == 0 and cols % BLOCK == 0 and stream.shape[1] % 128 == 0 and rows % (8 * HALVES) == 0:
        return fused(nt, nd, HALVES, *arrays)
    return body(*arrays)


def solution(mesh):
    placed = (
        P(None, ("dp", "tp")),
        P("dp"),
        P(None, "dp", "tp"),
        P(None, "dp", None, "tp"),
        P(None, "dp"),
        P(None, "dp", "tp"),
        P(None, "dp", "tp"),
        P(None, None, "tp"),
        P(None, None, "tp"),
        P(None, None, "tp"),
        P(None, "tp"),
        P(None, "tp", "dp"),
    )
    return jax.shard_map(
        functools.partial(step, mesh.shape["tp"], mesh.shape["dp"]),
        mesh=mesh,
        in_specs=placed,
        out_specs=(P(None, ("dp", "tp")), P(None, "dp", "tp"), P(None, "dp", None, "tp")),
        check_vma=False,
    )
```

```python
import functools

import jax
import jax.numpy as jnp
from jax import lax
from jax.experimental import pallas as pl
from jax.experimental.pallas import tpu as pltpu
from jax.sharding import PartitionSpec as P

D = 4096
BLOCK = 256


epsilon = 1e-06


def from_partner(block, axis, apart):
    count = lax.axis_size(axis)
    route = []
    for low in range(count):
        high = low | 1 << apart
        if high != low and high < count:
            route += [(low, high), (high, low)]
    return lax.ppermute(block, axis, route)


def norm_rows(block_rows, gain_values, squares):
    scaling = lax.rsqrt(squares / D + epsilon)
    return (block_rows.astype(jnp.float32) * scaling * gain_values).astype(jnp.bfloat16)


def normed_input(stream_local, gain_block):
    own_width = stream_local.shape[1]
    offset = lax.axis_index("tp") * own_width
    widened = stream_local.astype(jnp.float32)
    squares = lax.psum(jnp.sum(widened * widened, axis=1, keepdims=True), ("tp", "dp"))
    own_gain = lax.dynamic_slice_in_dim(gain_block, offset, own_width, 0)
    result = lax.all_gather(norm_rows(stream_local, own_gain, squares), "tp", axis=1, tiled=True)
    return result


def peer_block(convolved):
    col_count = convolved.shape[1]
    group_size = max(BLOCK // col_count, 1)
    device = lax.axis_index("tp")
    grouped = convolved
    for bit_number in range(group_size.bit_length() - 1):
        partner = from_partner(grouped, "tp", bit_number)
        is_upper = device // (1 << bit_number) % 2 == 1
        grouped = jnp.where(
            is_upper,
            jnp.concatenate([partner, grouped], axis=1),
            jnp.concatenate([grouped, partner], axis=1),
        )
    return grouped


def block_gates(grouped, weight):
    row_count = grouped.shape[0]
    col_count = weight.shape[1]
    blocks = max(col_count // BLOCK, 1)
    block_cols = min(col_count, BLOCK)
    inputs = grouped.reshape(row_count, blocks, BLOCK)
    tables = weight.reshape(BLOCK, blocks, block_cols)
    mapped = jnp.einsum("rnk,knc->rnc", inputs, tables, preferred_element_type=jnp.float32)
    return mapped.reshape(row_count, col_count)


def recurrent_step(
    normed,
    lengths,
    prior_state,
    prior_window,
    w_branch,
    w_gate_branch,
    conv_taps,
    w_in_gate,
    w_rec_gate,
    decay_param,
    w_out,
    stream_local,
):
    col_count = w_branch.shape[1]
    summed = lax.psum_scatter(
        jnp.concatenate(
            [
                jnp.dot(normed, w_branch, preferred_element_type=jnp.float32),
                jnp.dot(normed, w_gate_branch, preferred_element_type=jnp.float32),
            ],
            axis=1,
        ).astype(jnp.bfloat16),
        "dp",
        scatter_dimension=0,
        tiled=True,
    ).astype(jnp.float32)
    branch = summed[:, :col_count].astype(jnp.bfloat16)
    gate_in = summed[:, col_count:].astype(jnp.bfloat16)
    depth = prior_window.shape[1]
    needed = depth + 1 - jnp.arange(depth, dtype=jnp.int32)
    living = lengths[:, None, None] >= needed[None, :, None]
    history = jnp.where(living, prior_window, jnp.zeros_like(prior_window))
    window = jnp.concatenate([history, branch[:, None, :]], axis=1)
    convolved = jnp.sum(
        window.astype(jnp.float32) * conv_taps.astype(jnp.float32)[None], axis=1
    ).astype(jnp.bfloat16)
    grouped = peer_block(convolved)
    input_gate = jax.nn.sigmoid(block_gates(grouped, w_in_gate))
    recur_gate = jax.nn.sigmoid(block_gates(grouped, w_rec_gate))
    log_keep = 8.0 * recur_gate * jax.nn.log_sigmoid(decay_param)
    keeping = jnp.exp(log_keep)
    feeding = jnp.sqrt(-jnp.expm1(2.0 * log_keep))
    earlier = jnp.where(lengths[:, None] >= 2, prior_state, jnp.zeros_like(prior_state))
    state = keeping * earlier + feeding * input_gate * convolved.astype(jnp.float32)
    readout = (state * jax.nn.gelu(gate_in.astype(jnp.float32))).astype(jnp.bfloat16)
    mixed = jnp.dot(
        lax.all_gather(readout, "dp", axis=0, tiled=True), w_out, preferred_element_type=jnp.float32
    )
    own_width = stream_local.shape[1]
    offset = lax.axis_index("tp") * own_width
    own_cols = lax.dynamic_slice_in_dim(mixed, offset, own_width, 1) + stream_local.astype(
        jnp.float32
    )
    terms = lax.dynamic_update_slice_in_dim(mixed, own_cols, offset, 1)
    return (terms, state, window[:, 1:])


def body(
    stream,
    lengths,
    prior_state,
    prior_window,
    norm_gain,
    w_branch,
    w_gate_branch,
    conv_taps,
    w_in_gate,
    w_rec_gate,
    decay_param,
    w_out,
):
    normed = normed_input(stream, norm_gain[0])
    terms, state_first, window_first = recurrent_step(
        normed,
        lengths,
        prior_state[0],
        prior_window[0],
        w_branch[0],
        w_gate_branch[0],
        conv_taps[0],
        w_in_gate[0],
        w_rec_gate[0],
        decay_param[0],
        w_out[0],
        stream,
    )
    carried = lax.psum(terms, "tp").astype(jnp.bfloat16)
    widened = carried.astype(jnp.float32)
    squares = lax.psum(jnp.sum(widened * widened, axis=1, keepdims=True), "dp")
    normed = norm_rows(carried, norm_gain[1], squares)
    own_width = stream.shape[1]
    first = lax.dynamic_slice_in_dim(carried, lax.axis_index("tp") * own_width, own_width, 1)
    terms, state_second, window_second = recurrent_step(
        normed,
        lengths,
        prior_state[1],
        prior_window[1],
        w_branch[1],
        w_gate_branch[1],
        conv_taps[1],
        w_in_gate[1],
        w_rec_gate[1],
        decay_param[1],
        w_out[1],
        first,
    )
    second = lax.psum_scatter(terms, "tp", scatter_dimension=1, tiled=True).astype(jnp.bfloat16)
    return (
        second,
        jnp.stack([state_first, state_second]),
        jnp.stack([window_first, window_second]),
    )


GROUPS = 2
MAIN_VMEM = 60 * 1024 * 1024
TAIL_VMEM = 4 * 1024 * 1024
MESH = pl.DeviceIdType.MESH


def negative_expm1(z):
    series = -z * (1.0 + z / 2.0 * (1.0 + z / 3.0 * (1.0 + z / 4.0 * (1.0 + z / 5.0))))
    return jnp.where(z > -0.1, series, 1.0 - jnp.exp(z))


def fused_kernel(
    nt,
    nd,
    groups,
    stream,
    lengths,
    prior_state,
    prior_window,
    norm_gain,
    w_branch,
    w_gate_branch,
    conv_taps,
    w_in_gate,
    w_rec_gate,
    decay_param,
    w_out,
    mix_o,
    state_o,
    state_m,
    hist_o,
    branch_o,
    branch_m,
    xg,
    xm,
    part,
    px,
    mx,
    ms,
    fo,
    fm,
    res,
    am,
    aux,
    len_v,
    state_v,
    win_v,
    gain_v,
    wp_v,
    taps_v,
    gates_v,
    decay_v,
    wo_v,
    in_sem,
    sent,
    xr,
    xr_m,
    px_r,
    ms_r,
    f_r,
    res_r,
    aux_r,
    wp_r,
    wo_r,
    gain_r,
    st_r,
    br_r,
):
    t = lax.axis_index("tp")
    d = lax.axis_index("dp")
    core = lax.rem(d, 2)
    mate = d + 1 - 2 * core
    across = lax.rem(d + 2, nd)
    corner = lax.rem(mate + 2, nd)
    layers = w_branch.shape[0]
    last = layers - 1
    rows, own = stream.shape[1], stream.shape[2]
    r = rows // (2 * groups)
    full = nd * r
    cols = w_branch.shape[2]
    width = w_branch.shape[1]
    depth = prior_window.shape[1]

    barrier = pltpu.get_barrier_semaphore()
    tp_peers = [(k, flipped(t, k, nt)) for k in range(nt - 1, 0, -1)]
    for _, peer in tp_peers:
        for other in (d, mate):
            pl.semaphore_signal(
                barrier, inc=1, device_id={"tp": peer, "dp": other}, device_id_type=MESH
            )
    for peer in (across, corner, mate):
        pl.semaphore_signal(barrier, inc=1, device_id={"dp": peer}, device_id_type=MESH)

    counter = [0]

    def load(*pairs):
        sem = in_sem.at[counter[0]]
        counter[0] += 1
        for src, dst in pairs:
            pltpu.make_async_copy(src, dst, sem).start()
        return sem

    def loaded(ref, sem):
        pltpu.make_async_copy(ref, ref, sem).wait()

    def span(k, i):
        side = core if k == 0 else 1 - core
        return pl.ds(pl.multiple_of((side * groups + i) * r, r), r)

    c_own = [load((stream.at[:, span(0, i), :], xg.at[0, i, t, 0])) for i in range(groups)]
    c_mate = load(*[(stream.at[:, span(1, i), :], xm.at[i]) for i in range(groups)])
    c_gain = load((norm_gain, gain_v.at[0]))
    c_first = [
        (held, load((src, held)))
        for src, held in (
            (lengths, len_v),
            (conv_taps, taps_v),
            (prior_window, win_v),
            (prior_state, state_v),
        )
    ]
    c_w, c_o = [], []
    for l in range(layers):
        c_w.append(load((w_branch.at[l], wp_v.at[l, 0, 0]), (w_gate_branch.at[l], wp_v.at[l, 0, 1])))
        c_o.append(load((w_out.at[l], wo_v.at[l, 0])))
        if l == 0:
            c_gates = load((w_in_gate, gates_v.at[0]), (w_rec_gate, gates_v.at[1]))
            c_decay = load((decay_param, decay_v))

    kinds = {}

    def remote(src, dst, ssem, rsem, where):
        return pltpu.make_async_remote_copy(
            src_ref=src,
            dst_ref=dst,
            send_sem=ssem,
            recv_sem=rsem,
            device_id=where,
            device_id_type=MESH,
        )

    def send(src, dst, kind, rsem, where):
        ssem = sent.at[kinds.setdefault(kind, len(kinds))]
        remote(src, dst, ssem, rsem, where).start()

    def arrived(ref, rsem):
        remote(ref, ref, sent.at[0], rsem, {"dp": mate}).wait_recv()

    def all_sent(kind, ref):
        sem = sent.at[kinds[kind]]
        remote(ref, ref, sem, sem, {"dp": mate}).wait_send()

    def prepare():
        length = jnp.sum(
            jnp.where(
                lax.broadcasted_iota(jnp.int32, (rows, rows), 0)
                == lax.broadcasted_iota(jnp.int32, (rows, rows), 1),
                jnp.broadcast_to(len_v[...].astype(jnp.float32), (rows, rows)),
                0.0,
            ),
            axis=1,
            keepdims=True,
        )
        for l in range(layers):
            taps = taps_v[l].astype(jnp.float32)
            before = jnp.zeros((rows, cols), jnp.float32)
            for m in range(depth):
                row = win_v[l, m].astype(jnp.float32)
                row = jnp.where(length >= depth + 1 - m, row, 0.0)
                before = before + row * taps[m : m + 1]
                if m > 0:
                    hist_o[l, m - 1] = row.astype(jnp.bfloat16)
            earlier = jnp.where(length >= 2, state_v[l], 0.0)
            for k in range(2):
                for i in range(groups):
                    piece = slice((k * groups + i) * r, (k * groups + i + 1) * r)
                    am[l, k, i, 0] = before[piece]
                    am[l, k, i, 1] = earlier[piece]
            aux[l, d] = am[l, core]

    def send_history(l):
        send(am.at[l, core], aux.at[l, d], "aux", aux_r.at[l], {"dp": across})
        send(am.at[l, 1 - core], aux.at[l, d], "aux", aux_r.at[l], {"dp": corner})
        send(am.at[l, 1 - core], aux.at[l, d], "aux", aux_r.at[l], {"dp": mate})

    def send_weights(l):
        loaded(wp_v.at[l, 0], c_w[l])
        send(wp_v.at[l, 0], wp_v.at[l, 1], "wp", wp_r.at[l], {"dp": mate})

    def send_out(l):
        loaded(wo_v.at[l, 0], c_o[l])
        send(wo_v.at[l, 0], wo_v.at[l, 1], "wo", wo_r.at[l], {"dp": mate})

    def project(l, i):
        if l == 0:
            arrived(xg.at[l, i, pl.ds(0, nt - 1), 0], xr.at[l, i])
            arrived(xg.at[l, i, :, 1], xr_m.at[i])
        else:
            arrived(xg.at[l, i, pl.ds(0, nt - 1)], xr.at[l, i])
        if i == 0 and l == 0:
            arrived(gain_v.at[1], gain_r.at[0])
        squares = jnp.zeros((full, own), jnp.float32)
        products = [None, None]
        for k in range(2):
            pieces = []
            for j in range(nt):
                x = xg[l, i, j, k].reshape(full, own).astype(jnp.float32)
                squares = squares + x * x
                gain = gain_v[k, l : l + 1, j * own : (j + 1) * own]
                pieces.append((x * gain).astype(jnp.bfloat16))
            normed = jnp.concatenate(pieces, axis=1)
            if i == 0 and k == 1:
                arrived(wp_v.at[l, 1], wp_r.at[l])
            for w in range(2):
                term = jnp.dot(normed, wp_v[l, k, w], preferred_element_type=jnp.float32)
                products[w] = term if k == 0 else products[w] + term
        total = jnp.sum(squares, axis=1, keepdims=True)
        high = total.astype(jnp.bfloat16).astype(jnp.float32)
        lane = lax.broadcasted_iota(jnp.int32, (full, 128), 1)
        part[l, i, :, 2 * cols :] = jnp.where(lane < 64, high, total - high).astype(jnp.bfloat16)
        for w in range(2):
            part[l, i, :, w * cols : (w + 1) * cols] = products[w].astype(jnp.bfloat16)
        send(part.at[l, i], px.at[l, i], "px", px_r.at[l, i], {"dp": across})

    def recur(l, i):
        if i == 0:
            if l == 0:
                loaded(gates_v, c_gates)
                loaded(decay_v, c_decay)
            arrived(aux.at[l, pl.ds(0, nd - 1)], aux_r.at[l])
        before = aux[l, :, i, 0].reshape(full, cols)
        earlier = aux[l, :, i, 1].reshape(full, cols)
        taps = taps_v[l].astype(jnp.float32)
        raw = decay_v[l : l + 1]
        log_decay = jnp.minimum(raw, 0.0) - jnp.log1p(jnp.exp(-jnp.abs(raw)))
        arrived(px.at[l, i], px_r.at[l, i])
        summed = part[l, i].astype(jnp.float32) + px[l, i].astype(jnp.float32)
        squares = summed[:, 2 * cols : 2 * cols + 1] + summed[:, 2 * cols + 64 : 2 * cols + 65]
        scaling = lax.rsqrt(squares / (width * nd) + epsilon)
        branch = (summed[:, :cols] * scaling).astype(jnp.bfloat16)
        gate_in = (summed[:, cols : 2 * cols] * scaling).astype(jnp.bfloat16)
        branch_o[l, i] = branch.reshape(nd, r, cols)
        convolved = (before + branch.astype(jnp.float32) * taps[depth : depth + 1]).astype(
            jnp.bfloat16
        )
        mapped = []
        for w in range(2):
            mapped.append(
                jnp.concatenate(
                    [
                        jnp.dot(
                            convolved[:, n * BLOCK : (n + 1) * BLOCK],
                            gates_v[w, l, :, n * BLOCK : (n + 1) * BLOCK],
                            preferred_element_type=jnp.float32,
                        )
                        for n in range(cols // BLOCK)
                    ],
                    axis=1,
                )
            )
        input_gate = jax.nn.sigmoid(mapped[0])
        recur_gate = jax.nn.sigmoid(mapped[1])
        log_keep = 8.0 * recur_gate * log_decay
        feeding = jnp.sqrt(negative_expm1(2.0 * log_keep))
        state = jnp.exp(log_keep) * earlier + feeding * input_gate * convolved.astype(jnp.float32)
        state_o[l, i] = state.reshape(nd, r, cols)
        readout = (state * jax.nn.gelu(gate_in.astype(jnp.float32))).astype(jnp.bfloat16)
        return readout

    def mix(l, i, readout):
        for k in range(2):
            if i == 0 and k == 1:
                arrived(wo_v.at[l, 1], wo_r.at[l])
            mixed = jnp.dot(readout, wo_v[l, k], preferred_element_type=jnp.float32)
            for j in range(nt):
                mx[l, i, j, k] = mixed[:, j * own : (j + 1) * own].astype(jnp.bfloat16)
        for k, peer in tp_peers:
            if l < last:
                send(mx.at[l, i, peer], ms.at[l, i, k - 1], "ms", ms_r.at[l, i], {"tp": peer})
            else:
                send(mx.at[l, i, peer, 0], fo.at[i, k - 1], "fo", f_r.at[0, i], {"tp": peer})
                send(
                    mx.at[l, i, peer, 1],
                    fm.at[i, k],
                    "fm",
                    f_r.at[1, i],
                    {"tp": peer, "dp": mate},
                )
        if l == last:
            send(mx.at[l, i, t, 1], fm.at[i, 0], "fm", f_r.at[1, i], {"dp": mate})
        send(state_o.at[l, i, mate], state_m.at[l, i], "state", st_r.at[0], {"dp": mate})
        send(branch_o.at[l, i, mate], branch_m.at[l, i], "branch", br_r.at[0], {"dp": mate})

    def collect(l, i):
        arrived(ms.at[l, i], ms_r.at[l, i])
        for k in range(2):
            total = mx[l, i, t, k].astype(jnp.float32)
            total = total + xg[l, i, t, k].reshape(full, own).astype(jnp.float32)
            for j in range(nt - 1):
                total = total + ms[l, i, j, k].astype(jnp.float32)
            xg[l + 1, i, t, k] = total.astype(jnp.bfloat16).reshape(nd, r, own)
        block = xg.at[l + 1, i, t]
        for _, peer in tp_peers:
            send(block, block, "xg", xr.at[l + 1, i], {"tp": peer})
        if l + 1 == last:
            send(block.at[1], res.at[i], "res", res_r.at[i], {"dp": mate})

    def finish(k, i):
        if k == 0:
            total = mx[last, i, t, 0].astype(jnp.float32)
            total = total + xg[last, i, t, 0].reshape(full, own).astype(jnp.float32)
            held = fo
        else:
            arrived(res.at[i], res_r.at[i])
            total = res[i].reshape(full, own).astype(jnp.float32)
            held = fm
        arrived(held.at[i], f_r.at[k, i])
        for j in range(held.shape[1]):
            total = total + held[i, j].astype(jnp.float32)
        mix_o[k, i] = total.astype(jnp.bfloat16).reshape(nd, r, own)

    for i in range(groups):
        loaded(xg.at[0, i, t, 0], c_own[i])
    loaded(xm, c_mate)
    pl.semaphore_wait(barrier, 2 * (nt - 1) + 3)
    for i in range(groups):
        block = xg.at[0, i, t, 0]
        for _, peer in tp_peers:
            send(block, block, "xo", xr.at[0, i], {"tp": peer})
            send(xm.at[i], xg.at[0, i, t, 1], "xm", xr_m.at[i], {"tp": peer, "dp": mate})
        send(xm.at[i], xg.at[0, i, t, 1], "xm", xr_m.at[i], {"dp": mate})
    loaded(gain_v.at[0], c_gain)
    send(gain_v.at[0], gain_v.at[1], "gain", gain_r.at[0], {"dp": mate})
    send_weights(0)
    for ref, sem in c_first:
        loaded(ref, sem)
    prepare()
    send_history(0)
    send_out(0)
    for l in range(layers):
        for i in range(groups):
            project(l, i)
        if l + 1 < layers:
            send_weights(l + 1)
        for i in range(groups):
            readout = recur(l, i)
            mix(l, i, readout)
        if l + 1 < layers:
            send_history(l + 1)
            send_out(l + 1)
            for i in range(groups):
                collect(l, i)
    for i in range(groups):
        finish(0, i)
        finish(1, i)
    arrived(state_m, st_r.at[0])
    arrived(branch_m, br_r.at[0])
    all_sent("xo", xg.at[0, :, pl.ds(0, nt - 1), 0])
    all_sent("xm", xg.at[0, :, :, 1])
    all_sent("gain", gain_v.at[1])
    all_sent("wp", wp_v.at[:, 1])
    all_sent("wo", wo_v.at[:, 1])
    all_sent("aux", aux.at[:, pl.ds(0, nd - 1)])
    all_sent("px", px)
    all_sent("ms", ms)
    all_sent("xg", xg.at[pl.ds(1, last), :, pl.ds(0, nt - 1)])
    all_sent("res", res)
    all_sent("fo", fo)
    all_sent("fm", fm)
    all_sent("state", state_m)
    all_sent("branch", branch_m)


def flipped(index, mask, count):
    for bit in range(count.bit_length() - 1):
        if mask >> bit & 1:
            index = index + (1 << bit) * (1 - 2 * (index // (1 << bit) % 2))
    return index


def tail_kernel(
    mixed, state, state_m, hist, branch, branch_m, mixed_out, state_out, window_out, sem
):
    d = lax.axis_index("dp")
    core = lax.rem(d, 2)
    layers, depth = window_out.shape[:2]
    groups, r = mixed.shape[1], mixed.shape[3]

    def span(k, i):
        side = core if k == 0 else 1 - core
        return pl.ds(pl.multiple_of((side * groups + i) * r, r), r)

    pairs = []
    for i in range(groups):
        for k in range(2):
            pairs.append((mixed.at[k, i], mixed_out.at[:, span(k, i), :]))
    for l in range(layers):
        pairs.append((hist.at[l], window_out.at[l, pl.ds(0, depth - 1)]))
        for i in range(groups):
            pairs.append((state.at[l, i, d], state_out.at[l, span(0, i), :]))
            pairs.append((state_m.at[l, i], state_out.at[l, span(1, i), :]))
            pairs.append((branch.at[l, i, d], window_out.at[l, depth - 1, span(0, i), :]))
            pairs.append((branch_m.at[l, i], window_out.at[l, depth - 1, span(1, i), :]))
    stores = [pltpu.make_async_copy(src, dst, sem.at[k]) for k, (src, dst) in enumerate(pairs)]
    for copy in stores:
        copy.start()
    for copy in stores:
        copy.wait()


def fused(
    nt,
    nd,
    groups,
    stream,
    lengths,
    prior_state,
    prior_window,
    norm_gain,
    w_branch,
    w_gate_branch,
    conv_taps,
    w_in_gate,
    w_rec_gate,
    decay_param,
    w_out,
):
    layers, width, cols = w_branch.shape
    batch, own = stream.shape
    rows = batch // nd
    r = rows // (2 * groups)
    full = nd * r
    depth = prior_window.shape[2]
    window = prior_window.transpose(0, 2, 1, 3)
    bf16, f32 = jnp.bfloat16, jnp.float32
    anywhere = pl.BlockSpec(memory_space=pl.ANY)
    held = pl.BlockSpec(memory_space=pltpu.VMEM)
    dma = pltpu.SemaphoreType.DMA
    finals = pl.pallas_call(
        functools.partial(fused_kernel, nt, nd, groups),
        out_shape=(
            pltpu.VMEM((2, groups, nd, r, own), bf16),
            pltpu.VMEM((layers, groups, nd, r, cols), f32),
            pltpu.VMEM((layers, groups, r, cols), f32),
            pltpu.VMEM((layers, depth - 1, rows, cols), bf16),
            pltpu.VMEM((layers, groups, nd, r, cols), bf16),
            pltpu.VMEM((layers, groups, r, cols), bf16),
        ),
        in_specs=[pl.BlockSpec(memory_space=pltpu.HBM)] * 12,
        out_specs=(held,) * 6,
        scratch_shapes=[
            pltpu.VMEM((layers, groups, nt, 2, nd, r, own), bf16),
            pltpu.VMEM((groups, nd, r, own), bf16),
            pltpu.VMEM((layers, groups, full, 2 * cols + 128), bf16),
            pltpu.VMEM((layers, groups, full, 2 * cols + 128), bf16),
            pltpu.VMEM((layers, groups, nt, 2, full, own), bf16),
            pltpu.VMEM((layers - 1, groups, nt - 1, 2, full, own), bf16),
            pltpu.VMEM((groups, nt - 1, full, own), bf16),
            pltpu.VMEM((groups, nt, full, own), bf16),
            pltpu.VMEM((groups, nd, r, own), bf16),
            pltpu.VMEM((layers, 2, groups, 2, r, cols), f32),
            pltpu.VMEM((layers, nd, groups, 2, r, cols), f32),
            pltpu.VMEM((1, rows), jnp.int32),
            pltpu.VMEM(prior_state.shape, f32),
            pltpu.VMEM(window.shape, bf16),
            pltpu.VMEM((2,) + norm_gain.shape, f32),
            pltpu.VMEM((layers, 2, 2, width, cols), bf16),
            pltpu.VMEM(conv_taps.shape, bf16),
            pltpu.VMEM((2, layers, BLOCK, cols), bf16),
            pltpu.VMEM(decay_param.shape, f32),
            pltpu.VMEM((layers, 2, cols, width), bf16),
            dma((8 + groups + 2 * layers,)),
            dma((14,)),
            dma((layers, groups)),
            dma((groups,)),
            dma((layers, groups)),
            dma((layers - 1, groups)),
            dma((2, groups)),
            dma((groups,)),
            dma((layers,)),
            dma((layers,)),
            dma((layers,)),
            dma((1,)),
            dma((1,)),
            dma((1,)),
        ],
        compiler_params=pltpu.CompilerParams(
            collective_id=0, has_side_effects=True, vmem_limit_bytes=MAIN_VMEM
        ),
    )(
        stream.reshape(nd, rows, own),
        lengths.reshape(1, rows),
        prior_state,
        window,
        norm_gain,
        w_branch,
        w_gate_branch,
        conv_taps,
        w_in_gate,
        w_rec_gate,
        decay_param,
        w_out,
    )
    mixed, state, new_window = pl.pallas_call(
        tail_kernel,
        out_shape=(
            jax.ShapeDtypeStruct((nd, rows, own), bf16),
            jax.ShapeDtypeStruct(prior_state.shape, f32),
            jax.ShapeDtypeStruct(window.shape, bf16),
        ),
        in_specs=[held] * 6,
        out_specs=(anywhere,) * 3,
        scratch_shapes=[dma((2 * groups + layers * (1 + 4 * groups),))],
        compiler_params=pltpu.CompilerParams(vmem_limit_bytes=TAIL_VMEM),
    )(*finals)
    return mixed.reshape(batch, own), state, new_window.transpose(0, 2, 1, 3)


def step(nt, nd, *arrays):
    stream, w_branch = arrays[0], arrays[5]
    rows, cols = stream.shape[0] // nd, w_branch.shape[2]
    layers = w_branch.shape[0]
    if nd == 4 and layers > 1 and nt & (nt - 1) == 0 and cols % BLOCK == 0 and stream.shape[1] % 128 == 0 and rows % (16 * GROUPS) == 0:
        return fused(nt, nd, GROUPS, *arrays)
    return body(*arrays)


def solution(mesh):
    placed = (
        P(None, ("dp", "tp")),
        P("dp"),
        P(None, "dp", "tp"),
        P(None, "dp", None, "tp"),
        P(None, "dp"),
        P(None, "dp", "tp"),
        P(None, "dp", "tp"),
        P(None, None, "tp"),
        P(None, None, "tp"),
        P(None, None, "tp"),
        P(None, "tp"),
        P(None, "tp", "dp"),
    )
    return jax.shard_map(
        functools.partial(step, mesh.shape["tp"], mesh.shape["dp"]),
        mesh=mesh,
        in_specs=placed,
        out_specs=(P(None, ("dp", "tp")), P(None, "dp", "tp"), P(None, "dp", None, "tp")),
        check_vma=False,
    )
```

```python
import functools

import jax
import jax.numpy as jnp
from jax import lax
from jax.experimental import pallas as pl
from jax.experimental.pallas import tpu as pltpu
from jax.sharding import PartitionSpec as P

D = 4096
BLOCK = 256


epsilon = 1e-06


def from_partner(block, axis, apart):
    count = lax.axis_size(axis)
    route = []
    for low in range(count):
        high = low | 1 << apart
        if high != low and high < count:
            route += [(low, high), (high, low)]
    return lax.ppermute(block, axis, route)


def norm_rows(block_rows, gain_values, squares):
    scaling = lax.rsqrt(squares / D + epsilon)
    return (block_rows.astype(jnp.float32) * scaling * gain_values).astype(jnp.bfloat16)


def normed_input(stream_local, gain_block):
    own_width = stream_local.shape[1]
    offset = lax.axis_index("tp") * own_width
    widened = stream_local.astype(jnp.float32)
    squares = lax.psum(jnp.sum(widened * widened, axis=1, keepdims=True), ("tp", "dp"))
    own_gain = lax.dynamic_slice_in_dim(gain_block, offset, own_width, 0)
    result = lax.all_gather(norm_rows(stream_local, own_gain, squares), "tp", axis=1, tiled=True)
    return result


def peer_block(convolved):
    col_count = convolved.shape[1]
    group_size = max(BLOCK // col_count, 1)
    device = lax.axis_index("tp")
    grouped = convolved
    for bit_number in range(group_size.bit_length() - 1):
        partner = from_partner(grouped, "tp", bit_number)
        is_upper = device // (1 << bit_number) % 2 == 1
        grouped = jnp.where(
            is_upper,
            jnp.concatenate([partner, grouped], axis=1),
            jnp.concatenate([grouped, partner], axis=1),
        )
    return grouped


def block_gates(grouped, weight):
    row_count = grouped.shape[0]
    col_count = weight.shape[1]
    blocks = max(col_count // BLOCK, 1)
    block_cols = min(col_count, BLOCK)
    inputs = grouped.reshape(row_count, blocks, BLOCK)
    tables = weight.reshape(BLOCK, blocks, block_cols)
    mapped = jnp.einsum("rnk,knc->rnc", inputs, tables, preferred_element_type=jnp.float32)
    return mapped.reshape(row_count, col_count)


def recurrent_step(
    normed,
    lengths,
    prior_state,
    prior_window,
    w_branch,
    w_gate_branch,
    conv_taps,
    w_in_gate,
    w_rec_gate,
    decay_param,
    w_out,
    stream_local,
):
    col_count = w_branch.shape[1]
    summed = lax.psum_scatter(
        jnp.concatenate(
            [
                jnp.dot(normed, w_branch, preferred_element_type=jnp.float32),
                jnp.dot(normed, w_gate_branch, preferred_element_type=jnp.float32),
            ],
            axis=1,
        ).astype(jnp.bfloat16),
        "dp",
        scatter_dimension=0,
        tiled=True,
    ).astype(jnp.float32)
    branch = summed[:, :col_count].astype(jnp.bfloat16)
    gate_in = summed[:, col_count:].astype(jnp.bfloat16)
    depth = prior_window.shape[1]
    needed = depth + 1 - jnp.arange(depth, dtype=jnp.int32)
    living = lengths[:, None, None] >= needed[None, :, None]
    history = jnp.where(living, prior_window, jnp.zeros_like(prior_window))
    window = jnp.concatenate([history, branch[:, None, :]], axis=1)
    convolved = jnp.sum(
        window.astype(jnp.float32) * conv_taps.astype(jnp.float32)[None], axis=1
    ).astype(jnp.bfloat16)
    grouped = peer_block(convolved)
    input_gate = jax.nn.sigmoid(block_gates(grouped, w_in_gate))
    recur_gate = jax.nn.sigmoid(block_gates(grouped, w_rec_gate))
    log_keep = 8.0 * recur_gate * jax.nn.log_sigmoid(decay_param)
    keeping = jnp.exp(log_keep)
    feeding = jnp.sqrt(-jnp.expm1(2.0 * log_keep))
    earlier = jnp.where(lengths[:, None] >= 2, prior_state, jnp.zeros_like(prior_state))
    state = keeping * earlier + feeding * input_gate * convolved.astype(jnp.float32)
    readout = (state * jax.nn.gelu(gate_in.astype(jnp.float32))).astype(jnp.bfloat16)
    mixed = jnp.dot(
        lax.all_gather(readout, "dp", axis=0, tiled=True), w_out, preferred_element_type=jnp.float32
    )
    own_width = stream_local.shape[1]
    offset = lax.axis_index("tp") * own_width
    own_cols = lax.dynamic_slice_in_dim(mixed, offset, own_width, 1) + stream_local.astype(
        jnp.float32
    )
    terms = lax.dynamic_update_slice_in_dim(mixed, own_cols, offset, 1)
    return (terms, state, window[:, 1:])


def body(
    stream,
    lengths,
    prior_state,
    prior_window,
    norm_gain,
    w_branch,
    w_gate_branch,
    conv_taps,
    w_in_gate,
    w_rec_gate,
    decay_param,
    w_out,
):
    normed = normed_input(stream, norm_gain[0])
    terms, state_first, window_first = recurrent_step(
        normed,
        lengths,
        prior_state[0],
        prior_window[0],
        w_branch[0],
        w_gate_branch[0],
        conv_taps[0],
        w_in_gate[0],
        w_rec_gate[0],
        decay_param[0],
        w_out[0],
        stream,
    )
    carried = lax.psum(terms, "tp").astype(jnp.bfloat16)
    widened = carried.astype(jnp.float32)
    squares = lax.psum(jnp.sum(widened * widened, axis=1, keepdims=True), "dp")
    normed = norm_rows(carried, norm_gain[1], squares)
    own_width = stream.shape[1]
    first = lax.dynamic_slice_in_dim(carried, lax.axis_index("tp") * own_width, own_width, 1)
    terms, state_second, window_second = recurrent_step(
        normed,
        lengths,
        prior_state[1],
        prior_window[1],
        w_branch[1],
        w_gate_branch[1],
        conv_taps[1],
        w_in_gate[1],
        w_rec_gate[1],
        decay_param[1],
        w_out[1],
        first,
    )
    second = lax.psum_scatter(terms, "tp", scatter_dimension=1, tiled=True).astype(jnp.bfloat16)
    return (
        second,
        jnp.stack([state_first, state_second]),
        jnp.stack([window_first, window_second]),
    )


GROUPS = 2
MAIN_VMEM = 60 * 1024 * 1024
TAIL_VMEM = 4 * 1024 * 1024
MESH = pl.DeviceIdType.MESH


def negative_expm1(z):
    series = -z * (1.0 + z / 2.0 * (1.0 + z / 3.0 * (1.0 + z / 4.0 * (1.0 + z / 5.0))))
    return jnp.where(z > -0.1, series, 1.0 - jnp.exp(z))


def fused_kernel(
    nt,
    nd,
    groups,
    stream,
    lengths,
    prior_state,
    prior_window,
    norm_gain,
    w_branch,
    w_gate_branch,
    conv_taps,
    w_in_gate,
    w_rec_gate,
    decay_param,
    w_out,
    mix_o,
    state_o,
    state_m,
    hist_o,
    branch_o,
    branch_m,
    xg,
    xm,
    part,
    px,
    mx,
    ms,
    fo,
    fm,
    res,
    mq,
    rq,
    xq,
    am,
    aux,
    len_v,
    state_v,
    win_v,
    gain_v,
    wp_v,
    taps_v,
    gates_v,
    decay_v,
    wo_v,
    gain_s,
    acc,
    sq,
    in_sem,
    sent,
    xr,
    px_r,
    ms_r,
    f_r,
    res_r,
    mq_r,
    rq_r,
    aux_r,
    wp_r,
    wo_r,
    gain_r,
    st_r,
    br_r,
):
    t = lax.axis_index("tp")
    d = lax.axis_index("dp")
    core = lax.rem(d, 2)
    mate = d + 1 - 2 * core
    across = lax.rem(d + 2, nd)
    corner = lax.rem(mate + 2, nd)
    layers = w_branch.shape[0]
    last = layers - 1
    rows, own = stream.shape[1], stream.shape[2]
    r = rows // (2 * groups)
    full = nd * r
    cols = w_branch.shape[2]
    width = w_branch.shape[1]
    depth = prior_window.shape[1]

    halves_of = (pl.ds(0, 128 + cols), pl.ds(128 + cols, cols))

    barrier = pltpu.get_barrier_semaphore()
    tp_peers = [(k, flipped(t, k, nt)) for k in range(nt - 1, 0, -1)]
    for _, peer in tp_peers:
        for other in (d, mate):
            pl.semaphore_signal(
                barrier, inc=1, device_id={"tp": peer, "dp": other}, device_id_type=MESH
            )
    for peer in (across, corner, mate):
        pl.semaphore_signal(barrier, inc=1, device_id={"dp": peer}, device_id_type=MESH)

    counter = [0]

    def load(*pairs):
        sem = in_sem.at[counter[0]]
        counter[0] += 1
        for src, dst in pairs:
            pltpu.make_async_copy(src, dst, sem).start()
        return sem

    def loaded(ref, sem):
        pltpu.make_async_copy(ref, ref, sem).wait()

    def span(k, i):
        side = core if k == 0 else 1 - core
        return pl.ds(pl.multiple_of((side * groups + i) * r, r), r)

    c_own = [load((stream.at[:, span(0, i), :], xg.at[0, i, t, 0])) for i in range(groups)]
    c_mate = load(*[(stream.at[:, span(1, i), :], xm.at[i]) for i in range(groups)])
    c_gain = load((norm_gain, gain_v.at[0]))
    c_first = [
        (held, load((src, held)))
        for src, held in (
            (lengths, len_v),
            (conv_taps, taps_v),
            (prior_window, win_v),
            (prior_state, state_v),
        )
    ]
    c_w, c_o = [], []
    for l in range(layers):
        c_w.append(load((w_branch.at[l], wp_v.at[l, 0, 0]), (w_gate_branch.at[l], wp_v.at[l, 0, 1])))
        c_o.append(load((w_out.at[l], wo_v.at[l, 0])))
        if l == 0:
            c_gates = load((w_in_gate, gates_v.at[0]), (w_rec_gate, gates_v.at[1]))
            c_decay = load((decay_param, decay_v))

    kinds = {}

    def remote(src, dst, ssem, rsem, where):
        return pltpu.make_async_remote_copy(
            src_ref=src,
            dst_ref=dst,
            send_sem=ssem,
            recv_sem=rsem,
            device_id=where,
            device_id_type=MESH,
        )

    def send(src, dst, kind, rsem, where):
        ssem = sent.at[kinds.setdefault(kind, len(kinds))]
        remote(src, dst, ssem, rsem, where).start()

    def arrived(ref, rsem):
        remote(ref, ref, sent.at[0], rsem, {"dp": mate}).wait_recv()

    def all_sent(kind, ref):
        sem = sent.at[kinds[kind]]
        remote(ref, ref, sem, sem, {"dp": mate}).wait_send()

    def prepare():
        length = jnp.sum(
            jnp.where(
                lax.broadcasted_iota(jnp.int32, (rows, rows), 0)
                == lax.broadcasted_iota(jnp.int32, (rows, rows), 1),
                jnp.broadcast_to(len_v[...].astype(jnp.float32), (rows, rows)),
                0.0,
            ),
            axis=1,
            keepdims=True,
        )
        for l in range(layers):
            taps = taps_v[l].astype(jnp.float32)
            before = jnp.zeros((rows, cols), jnp.float32)
            for m in range(depth):
                row = win_v[l, m].astype(jnp.float32)
                row = jnp.where(length >= depth + 1 - m, row, 0.0)
                before = before + row * taps[m : m + 1]
                if m > 0:
                    hist_o[l, m - 1] = row.astype(jnp.bfloat16)
            earlier = jnp.where(length >= 2, state_v[l], 0.0)
            for k in range(2):
                for i in range(groups):
                    piece = slice((k * groups + i) * r, (k * groups + i + 1) * r)
                    am[l, k, i, 0] = before[piece]
                    am[l, k, i, 1] = earlier[piece]
            aux[l, d] = am[l, core]

    def send_history(l):
        send(am.at[l, core], aux.at[l, d], "aux", aux_r.at[l], {"dp": across})
        send(am.at[l, 1 - core], aux.at[l, d], "aux", aux_r.at[l], {"dp": corner})
        send(am.at[l, 1 - core], aux.at[l, d], "aux", aux_r.at[l], {"dp": mate})

    def send_weights(l):
        loaded(wp_v.at[l, 0], c_w[l])
        send(wp_v.at[l, 0], wp_v.at[l, 1], "wp", wp_r.at[l], {"dp": mate})

    def send_out(l):
        loaded(wo_v.at[l, 0], c_o[l])
        send(wo_v.at[l, 0], wo_v.at[l, 1], "wo", wo_r.at[l], {"dp": mate})

    def spread_gain(k):
        for l in range(layers):
            for j in range(nt):
                gain_s[k, l, j] = gain_v[k, l : l + 1, j * own : (j + 1) * own]

    def normed(l, i, k, first):
        squares = jnp.zeros((full, own), jnp.float32)
        pieces = []
        for j in range(nt // 2):
            x = xg[l, i, first + j, k].reshape(full, own).astype(jnp.float32)
            squares = squares + x * x
            pieces.append((x * gain_s[k, l, first + j]).astype(jnp.bfloat16))
        return jnp.concatenate(pieces, axis=1), squares

    def weight(l, k, w, first):
        return wp_v[l, k, w, pl.ds(pl.multiple_of(first * own, own * nt // 2), own * nt // 2), :]

    def project_near(l, i):
        if l == 0:
            arrived(xg.at[l, i, pl.ds(0, nt - 1), 0], xr.at[l, i, 0])
        else:

            @pl.when(core == 1)
            def _():
                arrived(xg.at[l, i, pl.ds(0, nt // 2 - 1)], xr.at[l, i, 0])

            @pl.when(core == 0)
            def _():
                arrived(xg.at[l, i, pl.ds(0, nt // 2)], xr.at[l, i, 0])

        if l < last:

            @pl.when(core == 0)
            def _():
                send(xg.at[l, i, t], rq.at[l, i], "rq", rq_r.at[l, i], {"dp": mate})

        first = t // (nt // 2) * (nt // 2)
        if i == 0 and l == 0:
            arrived(gain_v.at[1], gain_r.at[0])
            spread_gain(1)
        squares = []
        products = [None, None]
        for k in range(2):
            x, part_squares = normed(l, i, k, first)
            squares.append(part_squares)
            if i == 0 and k == 1:
                arrived(wp_v.at[l, 1], wp_r.at[l])
            for w in range(2):
                term = jnp.dot(x, weight(l, k, w, first), preferred_element_type=jnp.float32)
                products[w] = term if k == 0 else products[w] + term
        for w in range(2):
            acc[i, w] = products[w]
        sq[i] = squares[0] + squares[1]

    def project_far(l, i):
        arrived(xg.at[l, i, pl.ds(0, nt // 2)], xr.at[l, i, 1])
        first = (1 - t // (nt // 2)) * (nt // 2)
        x0, squares0 = normed(l, i, 0, first)
        x1, squares1 = normed(l, i, 1, first)
        total = jnp.sum(sq[i] + squares0 + squares1, axis=1, keepdims=True)
        high = total.astype(jnp.bfloat16).astype(jnp.float32)
        lane = lax.broadcasted_iota(jnp.int32, (full, 128), 1)
        part[l, i, :, :128] = jnp.where(lane < 64, high, total - high).astype(jnp.bfloat16)
        for w in range(2):
            product = acc[i, w] + jnp.dot(
                x0, weight(l, 0, w, first), preferred_element_type=jnp.float32
            )
            product = product + jnp.dot(
                x1, weight(l, 1, w, first), preferred_element_type=jnp.float32
            )
            part[l, i, :, 128 + w * cols : 128 + (w + 1) * cols] = product.astype(jnp.bfloat16)
            ready = halves_of[w]
            send(part.at[l, i, :, ready], px.at[l, i, :, ready], "px", px_r.at[l, i, w], {"dp": across})

    def recur(l, i):
        if i == 0:
            if l == 0:
                loaded(gates_v, c_gates)
                loaded(decay_v, c_decay)
            arrived(aux.at[l, pl.ds(0, nd - 1)], aux_r.at[l])
        before = aux[l, :, i, 0].reshape(full, cols)
        earlier = aux[l, :, i, 1].reshape(full, cols)
        taps = taps_v[l].astype(jnp.float32)
        raw = decay_v[l : l + 1]
        log_decay = jnp.minimum(raw, 0.0) - jnp.log1p(jnp.exp(-jnp.abs(raw)))
        first, second = halves_of
        arrived(px.at[l, i, :, first], px_r.at[l, i, 0])
        summed = part[l, i, :, first].astype(jnp.float32) + px[l, i, :, first].astype(jnp.float32)
        squares = summed[:, :1] + summed[:, 64:65]
        scaling = lax.rsqrt(squares / (width * nd) + epsilon)
        branch = (summed[:, 128:] * scaling).astype(jnp.bfloat16)
        branch_o[l, i] = branch.reshape(nd, r, cols)
        convolved = (before + branch.astype(jnp.float32) * taps[depth : depth + 1]).astype(
            jnp.bfloat16
        )
        mapped = []
        for w in range(2):
            mapped.append(
                jnp.concatenate(
                    [
                        jnp.dot(
                            convolved[:, n * BLOCK : (n + 1) * BLOCK],
                            gates_v[w, l, :, n * BLOCK : (n + 1) * BLOCK],
                            preferred_element_type=jnp.float32,
                        )
                        for n in range(cols // BLOCK)
                    ],
                    axis=1,
                )
            )
        input_gate = jax.nn.sigmoid(mapped[0])
        recur_gate = jax.nn.sigmoid(mapped[1])
        log_keep = 8.0 * recur_gate * log_decay
        feeding = jnp.sqrt(negative_expm1(2.0 * log_keep))
        state = jnp.exp(log_keep) * earlier + feeding * input_gate * convolved.astype(jnp.float32)
        state_o[l, i] = state.reshape(nd, r, cols)
        arrived(px.at[l, i, :, second], px_r.at[l, i, 1])
        summed = part[l, i, :, second].astype(jnp.float32) + px[l, i, :, second].astype(jnp.float32)
        gate_in = (summed * scaling).astype(jnp.bfloat16)
        readout = (state * jax.nn.gelu(gate_in.astype(jnp.float32))).astype(jnp.bfloat16)
        return readout

    def mix(l, i, readout):
        for k in range(2):
            if i == 0 and k == 1:
                arrived(wo_v.at[l, 1], wo_r.at[l])
            mixed = jnp.dot(readout, wo_v[l, k], preferred_element_type=jnp.float32)
            for j in range(nt):
                mx[l, i, j, k] = mixed[:, j * own : (j + 1) * own].astype(jnp.bfloat16)
            if l < last:

                @pl.when(core == 1)
                def _():
                    for n, peer in tp_peers:
                        block = mx.at[l, i, peer, k]
                        send(block, ms.at[l, i, n - 1, k], "ms", ms_r.at[l, i], {"tp": peer})

                @pl.when(core == 0)
                def _():
                    for n, peer in tp_peers:
                        block, where = mx.at[l, i, peer, k], {"tp": peer, "dp": mate}
                        send(block, mq.at[l, i, n, k], "mq", mq_r.at[l, i], where)
                    block = mx.at[l, i, t, k]
                    send(block, mq.at[l, i, 0, k], "mq", mq_r.at[l, i], {"dp": mate})

                continue
            for n, peer in tp_peers:
                block = mx.at[l, i, peer, k]
                if k == 0:
                    send(block, fo.at[i, n - 1], "fo", f_r.at[0, i], {"tp": peer})
                else:
                    send(block, fm.at[i, n], "fm", f_r.at[1, i], {"tp": peer, "dp": mate})
            if l == last and k == 1:
                send(mx.at[l, i, t, 1], fm.at[i, 0], "fm", f_r.at[1, i], {"dp": mate})
        send(state_o.at[l, i, mate], state_m.at[l, i], "state", st_r.at[0], {"dp": mate})
        send(branch_o.at[l, i, mate], branch_m.at[l, i], "branch", br_r.at[0], {"dp": mate})

    def collect(l, i):
        arrived(ms.at[l, i], ms_r.at[l, i])
        for k in range(2):
            total = mx[l, i, t, k].astype(jnp.float32)
            total = total + xg[l, i, t, k].reshape(full, own).astype(jnp.float32)
            for j in range(nt - 1):
                total = total + ms[l, i, j, k].astype(jnp.float32)
            xg[l + 1, i, t, k] = total.astype(jnp.bfloat16).reshape(nd, r, own)
        block = xg.at[l + 1, i, t]
        for n, peer in tp_peers:
            send(block, block, "xg", xr.at[l + 1, i, 2 * n // nt], {"tp": peer})
        if l + 1 == last:
            send(block.at[1], res.at[i], "res", res_r.at[i], {"dp": mate})

    def collect_mate(l, i):
        arrived(rq.at[l, i], rq_r.at[l, i])
        arrived(mq.at[l, i], mq_r.at[l, i])
        for k in range(2):
            total = rq[l, i, k].reshape(full, own).astype(jnp.float32)
            for j in range(nt):
                total = total + mq[l, i, j, k].astype(jnp.float32)
            xq[l, i, k] = total.astype(jnp.bfloat16).reshape(nd, r, own)
        block, dst = xq.at[l, i], xg.at[l + 1, i, t]
        for n, peer in tp_peers:
            send(block, dst, "xq", xr.at[l + 1, i, 2 * n // nt], {"tp": peer, "dp": mate})
        send(block, dst, "xq", xr.at[l + 1, i, 0], {"dp": mate})

    def finish(k, i):
        if k == 0:
            total = mx[last, i, t, 0].astype(jnp.float32)
            total = total + xg[last, i, t, 0].reshape(full, own).astype(jnp.float32)
            held = fo
        else:


            @pl.when(core == 0)
            def _():
                arrived(res.at[i], res_r.at[i])

            @pl.when(core == 1)
            def _():
                res[i] = xq[last - 1, i, 1]

            total = res[i].reshape(full, own).astype(jnp.float32)
            held = fm
        arrived(held.at[i], f_r.at[k, i])
        for j in range(held.shape[1]):
            total = total + held[i, j].astype(jnp.float32)
        mix_o[k, i] = total.astype(jnp.bfloat16).reshape(nd, r, own)

    for i in range(groups):
        loaded(xg.at[0, i, t, 0], c_own[i])
    loaded(xm, c_mate)
    pl.semaphore_wait(barrier, 2 * (nt - 1) + 3)
    def send_own(i):
        block = xg.at[0, i, t, 0]
        for n, peer in tp_peers:
            send(block, block, "xo", xr.at[0, i, 2 * n // nt], {"tp": peer})

    def send_mate(i):
        for n, peer in tp_peers:
            sem = xr.at[0, i, 2 * n // nt]
            send(xm.at[i], xg.at[0, i, t, 1], "xm", sem, {"tp": peer, "dp": mate})
        send(xm.at[i], xg.at[0, i, t, 1], "xm", xr.at[0, i, 0], {"dp": mate})

    for kind, calls in enumerate(((send_own, send_mate), (send_mate, send_own))):

        @pl.when(core == kind)
        def _():
            for i in range(groups):
                for call in calls:
                    call(i)

    loaded(gain_v.at[0], c_gain)
    send(gain_v.at[0], gain_v.at[1], "gain", gain_r.at[0], {"dp": mate})
    send_weights(0)
    for ref, sem in c_first:
        loaded(ref, sem)
    spread_gain(0)
    prepare()
    send_history(0)
    send_out(0)
    for l in range(layers):
        if l == 0:
            for i in range(groups):
                project_near(l, i)
        for i in range(groups):
            if l > 0:
                project_near(l, i)
            project_far(l, i)
        if l + 1 < layers:
            send_weights(l + 1)
        for i in range(groups):
            readout = recur(l, i)
            mix(l, i, readout)
        if l + 1 < layers:
            send_history(l + 1)
            send_out(l + 1)


            @pl.when(core == 1)
            def _():
                for i in range(groups):
                    collect(l, i)
                    collect_mate(l, i)

    for i in range(groups):
        finish(0, i)
        finish(1, i)
    arrived(state_m, st_r.at[0])
    arrived(branch_m, br_r.at[0])
    all_sent("xo", xg.at[0, :, pl.ds(0, nt - 1), 0])
    all_sent("xm", xg.at[0, :, :, 1])
    all_sent("gain", gain_v.at[1])
    all_sent("wp", wp_v.at[:, 1])
    all_sent("wo", wo_v.at[:, 1])
    all_sent("aux", aux.at[:, pl.ds(0, nd - 1)])
    all_sent("px", px)

    @pl.when(core == 1)
    def _():
        all_sent("ms", ms)
        all_sent("xg", xg.at[pl.ds(1, last), :, pl.ds(0, nt - 1)])
        all_sent("xq", xg.at[pl.ds(1, last)])
        all_sent("res", res)

    @pl.when(core == 0)
    def _():
        all_sent("mq", mq)
        all_sent("rq", rq)

    all_sent("fo", fo)
    all_sent("fm", fm)
    all_sent("state", state_m)
    all_sent("branch", branch_m)


def flipped(index, mask, count):
    for bit in range(count.bit_length() - 1):
        if mask >> bit & 1:
            index = index + (1 << bit) * (1 - 2 * (index // (1 << bit) % 2))
    return index


def tail_kernel(
    mixed, state, state_m, hist, branch, branch_m, mixed_out, state_out, window_out, sem
):
    d = lax.axis_index("dp")
    core = lax.rem(d, 2)
    layers, depth = window_out.shape[:2]
    groups, r = mixed.shape[1], mixed.shape[3]

    def span(k, i):
        side = core if k == 0 else 1 - core
        return pl.ds(pl.multiple_of((side * groups + i) * r, r), r)

    pairs = []
    for i in range(groups):
        for k in range(2):
            pairs.append((mixed.at[k, i], mixed_out.at[:, span(k, i), :]))
    for l in range(layers):
        pairs.append((hist.at[l], window_out.at[l, pl.ds(0, depth - 1)]))
        for i in range(groups):
            pairs.append((state.at[l, i, d], state_out.at[l, span(0, i), :]))
            pairs.append((state_m.at[l, i], state_out.at[l, span(1, i), :]))
            pairs.append((branch.at[l, i, d], window_out.at[l, depth - 1, span(0, i), :]))
            pairs.append((branch_m.at[l, i], window_out.at[l, depth - 1, span(1, i), :]))
    stores = [pltpu.make_async_copy(src, dst, sem.at[k]) for k, (src, dst) in enumerate(pairs)]
    for copy in stores:
        copy.start()
    for copy in stores:
        copy.wait()


def fused(
    nt,
    nd,
    groups,
    stream,
    lengths,
    prior_state,
    prior_window,
    norm_gain,
    w_branch,
    w_gate_branch,
    conv_taps,
    w_in_gate,
    w_rec_gate,
    decay_param,
    w_out,
):
    layers, width, cols = w_branch.shape
    batch, own = stream.shape
    rows = batch // nd
    r = rows // (2 * groups)
    full = nd * r
    depth = prior_window.shape[2]
    window = prior_window.transpose(0, 2, 1, 3)
    bf16, f32 = jnp.bfloat16, jnp.float32
    anywhere = pl.BlockSpec(memory_space=pl.ANY)
    held = pl.BlockSpec(memory_space=pltpu.VMEM)
    dma = pltpu.SemaphoreType.DMA
    finals = pl.pallas_call(
        functools.partial(fused_kernel, nt, nd, groups),
        out_shape=(
            pltpu.VMEM((2, groups, nd, r, own), bf16),
            pltpu.VMEM((layers, groups, nd, r, cols), f32),
            pltpu.VMEM((layers, groups, r, cols), f32),
            pltpu.VMEM((layers, depth - 1, rows, cols), bf16),
            pltpu.VMEM((layers, groups, nd, r, cols), bf16),
            pltpu.VMEM((layers, groups, r, cols), bf16),
        ),
        in_specs=[pl.BlockSpec(memory_space=pltpu.HBM)] * 12,
        out_specs=(held,) * 6,
        scratch_shapes=[
            pltpu.VMEM((layers, groups, nt, 2, nd, r, own), bf16),
            pltpu.VMEM((groups, nd, r, own), bf16),
            pltpu.VMEM((layers, groups, full, 2 * cols + 128), bf16),
            pltpu.VMEM((layers, groups, full, 2 * cols + 128), bf16),
            pltpu.VMEM((layers, groups, nt, 2, full, own), bf16),
            pltpu.VMEM((layers - 1, groups, nt - 1, 2, full, own), bf16),
            pltpu.VMEM((groups, nt - 1, full, own), bf16),
            pltpu.VMEM((groups, nt, full, own), bf16),
            pltpu.VMEM((groups, nd, r, own), bf16),
            pltpu.VMEM((layers - 1, groups, nt, 2, full, own), bf16),
            pltpu.VMEM((layers - 1, groups, 2, nd, r, own), bf16),
            pltpu.VMEM((layers - 1, groups, 2, nd, r, own), bf16),
            pltpu.VMEM((layers, 2, groups, 2, r, cols), f32),
            pltpu.VMEM((layers, nd, groups, 2, r, cols), f32),
            pltpu.VMEM((1, rows), jnp.int32),
            pltpu.VMEM(prior_state.shape, f32),
            pltpu.VMEM(window.shape, bf16),
            pltpu.VMEM((2,) + norm_gain.shape, f32),
            pltpu.VMEM((layers, 2, 2, width, cols), bf16),
            pltpu.VMEM(conv_taps.shape, bf16),
            pltpu.VMEM((2, layers, BLOCK, cols), bf16),
            pltpu.VMEM(decay_param.shape, f32),
            pltpu.VMEM((layers, 2, cols, width), bf16),
            pltpu.VMEM((2, layers, nt, 1, own), f32),
            pltpu.VMEM((groups, 2, full, cols), f32),
            pltpu.VMEM((groups, full, own), f32),
            dma((8 + groups + 2 * layers,)),
            dma((17,)),
            dma((layers, groups, 2)),
            dma((layers, groups, 2)),
            dma((layers - 1, groups)),
            dma((2, groups)),
            dma((groups,)),
            dma((layers - 1, groups)),
            dma((layers - 1, groups)),
            dma((layers,)),
            dma((layers,)),
            dma((layers,)),
            dma((1,)),
            dma((1,)),
            dma((1,)),
        ],
        compiler_params=pltpu.CompilerParams(
            collective_id=0, has_side_effects=True, vmem_limit_bytes=MAIN_VMEM
        ),
    )(
        stream.reshape(nd, rows, own),
        lengths.reshape(1, rows),
        prior_state,
        window,
        norm_gain,
        w_branch,
        w_gate_branch,
        conv_taps,
        w_in_gate,
        w_rec_gate,
        decay_param,
        w_out,
    )
    mixed, state, new_window = pl.pallas_call(
        tail_kernel,
        out_shape=(
            jax.ShapeDtypeStruct((nd, rows, own), bf16),
            jax.ShapeDtypeStruct(prior_state.shape, f32),
            jax.ShapeDtypeStruct(window.shape, bf16),
        ),
        in_specs=[held] * 6,
        out_specs=(anywhere,) * 3,
        scratch_shapes=[dma((2 * groups + layers * (1 + 4 * groups),))],
        compiler_params=pltpu.CompilerParams(vmem_limit_bytes=TAIL_VMEM),
    )(*finals)
    return mixed.reshape(batch, own), state, new_window.transpose(0, 2, 1, 3)


def step(nt, nd, *arrays):
    stream, w_branch = arrays[0], arrays[5]
    rows, cols = stream.shape[0] // nd, w_branch.shape[2]
    layers = w_branch.shape[0]
    if nd == 4 and layers > 1 and nt & (nt - 1) == 0 and cols % BLOCK == 0 and stream.shape[1] % 128 == 0 and rows % (16 * GROUPS) == 0:
        return fused(nt, nd, GROUPS, *arrays)
    return body(*arrays)


def solution(mesh):
    placed = (
        P(None, ("dp", "tp")),
        P("dp"),
        P(None, "dp", "tp"),
        P(None, "dp", None, "tp"),
        P(None, "dp"),
        P(None, "dp", "tp"),
        P(None, "dp", "tp"),
        P(None, None, "tp"),
        P(None, None, "tp"),
        P(None, None, "tp"),
        P(None, "tp"),
        P(None, "tp", "dp"),
    )
    return jax.shard_map(
        functools.partial(step, mesh.shape["tp"], mesh.shape["dp"]),
        mesh=mesh,
        in_specs=placed,
        out_specs=(P(None, ("dp", "tp")), P(None, "dp", "tp"), P(None, "dp", None, "tp")),
        check_vma=False,
    )
```

```python
import functools

import jax
import jax.numpy as jnp
from jax import lax
from jax.experimental import pallas as pl
from jax.experimental.pallas import tpu as pltpu
from jax.sharding import PartitionSpec as P

D = 4096
BLOCK = 256


epsilon = 1e-06


def from_partner(block, axis, apart):
    count = lax.axis_size(axis)
    route = []
    for low in range(count):
        high = low | 1 << apart
        if high != low and high < count:
            route += [(low, high), (high, low)]
    return lax.ppermute(block, axis, route)


def norm_rows(block_rows, gain_values, squares):
    scaling = lax.rsqrt(squares / D + epsilon)
    return (block_rows.astype(jnp.float32) * scaling * gain_values).astype(jnp.bfloat16)


def normed_input(stream_local, gain_block):
    own_width = stream_local.shape[1]
    offset = lax.axis_index("tp") * own_width
    widened = stream_local.astype(jnp.float32)
    squares = lax.psum(jnp.sum(widened * widened, axis=1, keepdims=True), ("tp", "dp"))
    own_gain = lax.dynamic_slice_in_dim(gain_block, offset, own_width, 0)
    result = lax.all_gather(norm_rows(stream_local, own_gain, squares), "tp", axis=1, tiled=True)
    return result


def peer_block(convolved):
    col_count = convolved.shape[1]
    group_size = max(BLOCK // col_count, 1)
    device = lax.axis_index("tp")
    grouped = convolved
    for bit_number in range(group_size.bit_length() - 1):
        partner = from_partner(grouped, "tp", bit_number)
        is_upper = device // (1 << bit_number) % 2 == 1
        grouped = jnp.where(
            is_upper,
            jnp.concatenate([partner, grouped], axis=1),
            jnp.concatenate([grouped, partner], axis=1),
        )
    return grouped


def block_gates(grouped, weight):
    row_count = grouped.shape[0]
    col_count = weight.shape[1]
    blocks = max(col_count // BLOCK, 1)
    block_cols = min(col_count, BLOCK)
    inputs = grouped.reshape(row_count, blocks, BLOCK)
    tables = weight.reshape(BLOCK, blocks, block_cols)
    mapped = jnp.einsum("rnk,knc->rnc", inputs, tables, preferred_element_type=jnp.float32)
    return mapped.reshape(row_count, col_count)


def recurrent_step(
    normed,
    lengths,
    prior_state,
    prior_window,
    w_branch,
    w_gate_branch,
    conv_taps,
    w_in_gate,
    w_rec_gate,
    decay_param,
    w_out,
    stream_local,
):
    col_count = w_branch.shape[1]
    summed = lax.psum_scatter(
        jnp.concatenate(
            [
                jnp.dot(normed, w_branch, preferred_element_type=jnp.float32),
                jnp.dot(normed, w_gate_branch, preferred_element_type=jnp.float32),
            ],
            axis=1,
        ).astype(jnp.bfloat16),
        "dp",
        scatter_dimension=0,
        tiled=True,
    ).astype(jnp.float32)
    branch = summed[:, :col_count].astype(jnp.bfloat16)
    gate_in = summed[:, col_count:].astype(jnp.bfloat16)
    depth = prior_window.shape[1]
    needed = depth + 1 - jnp.arange(depth, dtype=jnp.int32)
    living = lengths[:, None, None] >= needed[None, :, None]
    history = jnp.where(living, prior_window, jnp.zeros_like(prior_window))
    window = jnp.concatenate([history, branch[:, None, :]], axis=1)
    convolved = jnp.sum(
        window.astype(jnp.float32) * conv_taps.astype(jnp.float32)[None], axis=1
    ).astype(jnp.bfloat16)
    grouped = peer_block(convolved)
    input_gate = jax.nn.sigmoid(block_gates(grouped, w_in_gate))
    recur_gate = jax.nn.sigmoid(block_gates(grouped, w_rec_gate))
    log_keep = 8.0 * recur_gate * jax.nn.log_sigmoid(decay_param)
    keeping = jnp.exp(log_keep)
    feeding = jnp.sqrt(-jnp.expm1(2.0 * log_keep))
    earlier = jnp.where(lengths[:, None] >= 2, prior_state, jnp.zeros_like(prior_state))
    state = keeping * earlier + feeding * input_gate * convolved.astype(jnp.float32)
    readout = (state * jax.nn.gelu(gate_in.astype(jnp.float32))).astype(jnp.bfloat16)
    mixed = jnp.dot(
        lax.all_gather(readout, "dp", axis=0, tiled=True), w_out, preferred_element_type=jnp.float32
    )
    own_width = stream_local.shape[1]
    offset = lax.axis_index("tp") * own_width
    own_cols = lax.dynamic_slice_in_dim(mixed, offset, own_width, 1) + stream_local.astype(
        jnp.float32
    )
    terms = lax.dynamic_update_slice_in_dim(mixed, own_cols, offset, 1)
    return (terms, state, window[:, 1:])


def body(
    stream,
    lengths,
    prior_state,
    prior_window,
    norm_gain,
    w_branch,
    w_gate_branch,
    conv_taps,
    w_in_gate,
    w_rec_gate,
    decay_param,
    w_out,
):
    normed = normed_input(stream, norm_gain[0])
    terms, state_first, window_first = recurrent_step(
        normed,
        lengths,
        prior_state[0],
        prior_window[0],
        w_branch[0],
        w_gate_branch[0],
        conv_taps[0],
        w_in_gate[0],
        w_rec_gate[0],
        decay_param[0],
        w_out[0],
        stream,
    )
    carried = lax.psum(terms, "tp").astype(jnp.bfloat16)
    widened = carried.astype(jnp.float32)
    squares = lax.psum(jnp.sum(widened * widened, axis=1, keepdims=True), "dp")
    normed = norm_rows(carried, norm_gain[1], squares)
    own_width = stream.shape[1]
    first = lax.dynamic_slice_in_dim(carried, lax.axis_index("tp") * own_width, own_width, 1)
    terms, state_second, window_second = recurrent_step(
        normed,
        lengths,
        prior_state[1],
        prior_window[1],
        w_branch[1],
        w_gate_branch[1],
        conv_taps[1],
        w_in_gate[1],
        w_rec_gate[1],
        decay_param[1],
        w_out[1],
        first,
    )
    second = lax.psum_scatter(terms, "tp", scatter_dimension=1, tiled=True).astype(jnp.bfloat16)
    return (
        second,
        jnp.stack([state_first, state_second]),
        jnp.stack([window_first, window_second]),
    )


GROUPS = 2
MAIN_VMEM = 60 * 1024 * 1024
TAIL_VMEM = 4 * 1024 * 1024
MESH = pl.DeviceIdType.MESH


def negative_expm1(z):
    series = -z * (1.0 + z / 2.0 * (1.0 + z / 3.0 * (1.0 + z / 4.0 * (1.0 + z / 5.0))))
    return jnp.where(z > -0.1, series, 1.0 - jnp.exp(z))


def fused_kernel(
    nt,
    nd,
    groups,
    stream,
    lengths,
    prior_state,
    prior_window,
    norm_gain,
    w_branch,
    w_gate_branch,
    conv_taps,
    w_in_gate,
    w_rec_gate,
    decay_param,
    w_out,
    mix_o,
    state_o,
    state_m,
    hist_o,
    branch_o,
    branch_m,
    xg,
    xm,
    part,
    px,
    mx,
    ms,
    fo,
    fm,
    res,
    mq,
    rq,
    xq,
    zs,
    zr,
    am,
    aux,
    len_v,
    state_v,
    win_v,
    gain_v,
    wp_v,
    taps_v,
    gates_v,
    decay_v,
    wo_v,
    gain_s,
    acc,
    sq,
    in_sem,
    sent,
    xr,
    px_r,
    ms_r,
    f_r,
    res_r,
    mq_r,
    rq_r,
    z_r,
    aux_r,
    wp_r,
    wo_r,
    gain_r,
    st_r,
    br_r,
):
    t = lax.axis_index("tp")
    d = lax.axis_index("dp")
    core = lax.rem(d, 2)
    mate = d + 1 - 2 * core
    across = lax.rem(d + 2, nd)
    corner = lax.rem(mate + 2, nd)
    layers = w_branch.shape[0]
    last = layers - 1
    rows, own = stream.shape[1], stream.shape[2]
    r = rows // (2 * groups)
    full = nd * r
    cols = w_branch.shape[2]
    width = w_branch.shape[1]
    depth = prior_window.shape[1]

    half = nt // 2
    place = lax.rem(t, half)
    halves_of = (pl.ds(0, 128 + cols), pl.ds(128 + cols, cols))

    barrier = pltpu.get_barrier_semaphore()
    tp_peers = [(k, flipped(t, k, nt)) for k in range(nt - 1, 0, -1)]
    opposite = flipped(t, half, nt)
    tp_near = [(k, peer) for k, peer in tp_peers if k < half]
    for _, peer in tp_peers:
        for other in (d, mate):
            pl.semaphore_signal(
                barrier, inc=1, device_id={"tp": peer, "dp": other}, device_id_type=MESH
            )
    for peer in (across, corner, mate):
        pl.semaphore_signal(barrier, inc=1, device_id={"dp": peer}, device_id_type=MESH)

    counter = [0]

    def load(*pairs):
        sem = in_sem.at[counter[0]]
        counter[0] += 1
        for src, dst in pairs:
            pltpu.make_async_copy(src, dst, sem).start()
        return sem

    def loaded(ref, sem):
        pltpu.make_async_copy(ref, ref, sem).wait()

    def span(k, i):
        side = core if k == 0 else 1 - core
        return pl.ds(pl.multiple_of((side * groups + i) * r, r), r)

    c_own = [load((stream.at[:, span(0, i), :], xg.at[0, i, t, 0])) for i in range(groups)]
    c_mate = load(*[(stream.at[:, span(1, i), :], xm.at[i]) for i in range(groups)])
    c_gain = load((norm_gain, gain_v.at[0]))
    c_first = [
        (held, load((src, held)))
        for src, held in (
            (lengths, len_v),
            (conv_taps, taps_v),
            (prior_window, win_v),
            (prior_state, state_v),
        )
    ]
    c_w, c_o = [], []
    for l in range(layers):
        c_w.append(load((w_branch.at[l], wp_v.at[l, 0, 0]), (w_gate_branch.at[l], wp_v.at[l, 0, 1])))
        c_o.append(load((w_out.at[l], wo_v.at[l, 0])))
        if l == 0:
            c_gates = load((w_in_gate, gates_v.at[0]), (w_rec_gate, gates_v.at[1]))
            c_decay = load((decay_param, decay_v))

    kinds = {}

    def remote(src, dst, ssem, rsem, where):
        return pltpu.make_async_remote_copy(
            src_ref=src,
            dst_ref=dst,
            send_sem=ssem,
            recv_sem=rsem,
            device_id=where,
            device_id_type=MESH,
        )

    def send(src, dst, kind, rsem, where):
        ssem = sent.at[kinds.setdefault(kind, len(kinds))]
        remote(src, dst, ssem, rsem, where).start()

    def arrived(ref, rsem):
        remote(ref, ref, sent.at[0], rsem, {"dp": mate}).wait_recv()

    def all_sent(kind, ref):
        sem = sent.at[kinds[kind]]
        remote(ref, ref, sem, sem, {"dp": mate}).wait_send()

    def prepare():
        length = jnp.sum(
            jnp.where(
                lax.broadcasted_iota(jnp.int32, (rows, rows), 0)
                == lax.broadcasted_iota(jnp.int32, (rows, rows), 1),
                jnp.broadcast_to(len_v[...].astype(jnp.float32), (rows, rows)),
                0.0,
            ),
            axis=1,
            keepdims=True,
        )
        for l in range(layers):
            taps = taps_v[l].astype(jnp.float32)
            before = jnp.zeros((rows, cols), jnp.float32)
            for m in range(depth):
                row = win_v[l, m].astype(jnp.float32)
                row = jnp.where(length >= depth + 1 - m, row, 0.0)
                before = before + row * taps[m : m + 1]
                if m > 0:
                    hist_o[l, m - 1] = row.astype(jnp.bfloat16)
            earlier = jnp.where(length >= 2, state_v[l], 0.0)
            for k in range(2):
                for i in range(groups):
                    piece = slice((k * groups + i) * r, (k * groups + i + 1) * r)
                    am[l, k, i, 0] = before[piece]
                    am[l, k, i, 1] = earlier[piece]
            aux[l, d] = am[l, core]

    def send_history(l):
        send(am.at[l, core], aux.at[l, d], "aux", aux_r.at[l], {"dp": across})
        send(am.at[l, 1 - core], aux.at[l, d], "aux", aux_r.at[l], {"dp": corner})
        send(am.at[l, 1 - core], aux.at[l, d], "aux", aux_r.at[l], {"dp": mate})

    def send_weights(l):
        loaded(wp_v.at[l, 0], c_w[l])
        send(wp_v.at[l, 0], wp_v.at[l, 1], "wp", wp_r.at[l], {"dp": mate})

    def send_out(l):
        loaded(wo_v.at[l, 0], c_o[l])
        send(wo_v.at[l, 0], wo_v.at[l, 1], "wo", wo_r.at[l], {"dp": mate})

    def spread_gain(k):
        for l in range(layers):
            for j in range(nt):
                gain_s[k, l, j] = gain_v[k, l : l + 1, j * own : (j + 1) * own]

    def normed(l, i, k, first, count=nt // 2):
        squares = jnp.zeros((full, own), jnp.float32)
        pieces = []
        for j in range(count):
            x = xg[l, i, first + j, k].reshape(full, own).astype(jnp.float32)
            squares = squares + x * x
            pieces.append((x * gain_s[k, l, first + j]).astype(jnp.bfloat16))
        return jnp.concatenate(pieces, axis=1), squares

    def weight(l, k, w, first):
        return wp_v[l, k, w, pl.ds(pl.multiple_of(first * own, own * nt // 2), own * nt // 2), :]

    def project_near(l, i):
        arrived(xg.at[l, i, pl.ds(0, nt - 1), 0], xr.at[l, i, 0])
        first = t // (nt // 2) * (nt // 2)
        if i == 0:
            arrived(gain_v.at[1], gain_r.at[0])
            spread_gain(1)
        squares = []
        products = [None, None]
        for k in range(2):
            x, part_squares = normed(l, i, k, first)
            squares.append(part_squares)
            if i == 0 and k == 1:
                arrived(wp_v.at[l, 1], wp_r.at[l])
            for w in range(2):
                term = jnp.dot(x, weight(l, k, w, first), preferred_element_type=jnp.float32)
                products[w] = term if k == 0 else products[w] + term
        for w in range(2):
            acc[i, w] = products[w]
        sq[i] = squares[0] + squares[1]

    def project_far(l, i):
        arrived(xg.at[l, i, pl.ds(0, nt // 2)], xr.at[l, i, 1])
        send_before(l, i)
        first = (1 - t // (nt // 2)) * (nt // 2)
        x0, squares0 = normed(l, i, 0, first)
        x1, squares1 = normed(l, i, 1, first)
        publish(l, i, sq[i] + squares0 + squares1, x0, x1, first, nt // 2)

    def project_all(l, i):
        @pl.when(core == 1)
        def _():
            arrived(xg.at[l, i, pl.ds(0, 2 * half - 2)], xr.at[l, i, 0])

        @pl.when(core == 0)
        def _():
            arrived(xg.at[l, i], xr.at[l, i, 0])

        if l < last:
            send_before(l, i)
        x0, squares0 = normed(l, i, 0, 0, nt)
        x1, squares1 = normed(l, i, 1, 0, nt)
        if i == 0:
            arrived(wp_v.at[l, 1], wp_r.at[l])
        publish(l, i, squares0 + squares1, x0, x1, 0, nt)

    def send_before(l, i):
        @pl.when(core == 0)
        def _():
            for h in range(2):
                block = xg.at[l, i, h * half + place]
                send(block, rq.at[l, i, h], "rq", rq_r.at[l, i], {"dp": mate})

    def publish(l, i, squares, x0, x1, first, count):
        total = jnp.sum(squares, axis=1, keepdims=True)
        high = total.astype(jnp.bfloat16).astype(jnp.float32)
        lane = lax.broadcasted_iota(jnp.int32, (full, 128), 1)
        part[l, i, :, :128] = jnp.where(lane < 64, high, total - high).astype(jnp.bfloat16)
        for w in range(2):
            product = None
            for k, x in enumerate((x0, x1)):
                table = wp_v[l, k, w] if count == nt else weight(l, k, w, first)
                term = jnp.dot(x, table, preferred_element_type=jnp.float32)
                product = term if product is None else product + term
            if count < nt:
                product = product + acc[i, w]
            part[l, i, :, 128 + w * cols : 128 + (w + 1) * cols] = product.astype(jnp.bfloat16)
            ready = halves_of[w]
            send(part.at[l, i, :, ready], px.at[l, i, :, ready], "px", px_r.at[l, i, w], {"dp": across})

    def recur(l, i):
        if i == 0:
            if l == 0:
                loaded(gates_v, c_gates)
                loaded(decay_v, c_decay)
            arrived(aux.at[l, pl.ds(0, nd - 1)], aux_r.at[l])
        before = aux[l, :, i, 0].reshape(full, cols)
        earlier = aux[l, :, i, 1].reshape(full, cols)
        taps = taps_v[l].astype(jnp.float32)
        raw = decay_v[l : l + 1]
        log_decay = jnp.minimum(raw, 0.0) - jnp.log1p(jnp.exp(-jnp.abs(raw)))
        first, second = halves_of
        arrived(px.at[l, i, :, first], px_r.at[l, i, 0])
        summed = part[l, i, :, first].astype(jnp.float32) + px[l, i, :, first].astype(jnp.float32)
        squares = summed[:, :1] + summed[:, 64:65]
        scaling = lax.rsqrt(squares / (width * nd) + epsilon)
        branch = (summed[:, 128:] * scaling).astype(jnp.bfloat16)
        branch_o[l, i] = branch.reshape(nd, r, cols)
        convolved = (before + branch.astype(jnp.float32) * taps[depth : depth + 1]).astype(
            jnp.bfloat16
        )
        mapped = []
        for w in range(2):
            mapped.append(
                jnp.concatenate(
                    [
                        jnp.dot(
                            convolved[:, n * BLOCK : (n + 1) * BLOCK],
                            gates_v[w, l, :, n * BLOCK : (n + 1) * BLOCK],
                            preferred_element_type=jnp.float32,
                        )
                        for n in range(cols // BLOCK)
                    ],
                    axis=1,
                )
            )
        input_gate = jax.nn.sigmoid(mapped[0])
        recur_gate = jax.nn.sigmoid(mapped[1])
        log_keep = 8.0 * recur_gate * log_decay
        feeding = jnp.sqrt(negative_expm1(2.0 * log_keep))
        state = jnp.exp(log_keep) * earlier + feeding * input_gate * convolved.astype(jnp.float32)
        state_o[l, i] = state.reshape(nd, r, cols)
        arrived(px.at[l, i, :, second], px_r.at[l, i, 1])
        summed = part[l, i, :, second].astype(jnp.float32) + px[l, i, :, second].astype(jnp.float32)
        gate_in = (summed * scaling).astype(jnp.bfloat16)
        readout = (state * jax.nn.gelu(gate_in.astype(jnp.float32))).astype(jnp.bfloat16)
        return readout

    def mix(l, i, readout):
        for k in range(2):
            if i == 0 and k == 1:
                arrived(wo_v.at[l, 1], wo_r.at[l])
            mixed = jnp.dot(readout, wo_v[l, k], preferred_element_type=jnp.float32)
            for j in range(nt):
                mx[l, i, j, k] = mixed[:, j * own : (j + 1) * own].astype(jnp.bfloat16)
            if l < last:
                continue
            for n, peer in tp_peers:
                block = mx.at[l, i, peer, k]
                if k == 0:
                    send(block, fo.at[i, n - 1], "fo", f_r.at[0, i], {"tp": peer})
                else:
                    send(block, fm.at[i, n], "fm", f_r.at[1, i], {"tp": peer, "dp": mate})
            if l == last and k == 1:
                send(mx.at[l, i, t, 1], fm.at[i, 0], "fm", f_r.at[1, i], {"dp": mate})
        if l < last:

            @pl.when(core == 1)
            def _():
                for n, peer in tp_near:
                    for h in range(2):
                        block = mx.at[l, i, h * half + lax.rem(peer, half)]
                        send(block, ms.at[l, i, n - 1, h], "ms", ms_r.at[l, i], {"tp": peer})

            @pl.when(core == 0)
            def _():
                for n, peer in tp_near:
                    for h in range(2):
                        block = mx.at[l, i, h * half + lax.rem(peer, half)]
                        where = {"tp": peer, "dp": mate}
                        send(block, mq.at[l, i, n, h], "mq", mq_r.at[l, i], where)
                for h in range(2):
                    block = mx.at[l, i, h * half + place]
                    send(block, mq.at[l, i, 0, h], "mq", mq_r.at[l, i], {"dp": mate})

        send(state_o.at[l, i, mate], state_m.at[l, i], "state", st_r.at[0], {"dp": mate})
        send(branch_o.at[l, i, mate], branch_m.at[l, i], "branch", br_r.at[0], {"dp": mate})

    def collect(l, i):
        arrived(ms.at[l, i], ms_r.at[l, i])
        for h in range(2):
            for k in range(2):
                total = mx[l, i, h * half + place, k].astype(jnp.float32)
                for j in range(half - 1):
                    total = total + ms[l, i, j, h, k].astype(jnp.float32)
                zs[l, 0, i, h, k] = total.astype(jnp.bfloat16)
        send(zs.at[l, 0, i], zr.at[l, 0, i], "zs", z_r.at[l, 0, i], {"tp": opposite})

    def collect_mate(l, i):
        arrived(mq.at[l, i], mq_r.at[l, i])
        for h in range(2):
            for k in range(2):
                total = mq[l, i, 0, h, k].astype(jnp.float32)
                for j in range(1, half):
                    total = total + mq[l, i, j, h, k].astype(jnp.float32)
                zs[l, 1, i, h, k] = total.astype(jnp.bfloat16)
        send(zs.at[l, 1, i], zr.at[l, 1, i], "zs", z_r.at[l, 1, i], {"tp": opposite})

    def whole(l, which, i, h, k, before):
        total = zs[l, which, i, h, k].astype(jnp.float32) + zr[l, which, i, h, k].astype(jnp.float32)
        total = total + before.reshape(full, own).astype(jnp.float32)
        return total.astype(jnp.bfloat16).reshape(nd, r, own)

    def expand(l, i):
        arrived(zr.at[l, 0, i], z_r.at[l, 0, i])
        for h in range(2):
            for k in range(2):
                before = xg[l, i, h * half + place, k]
                xg[l + 1, i, h * half + place, k] = whole(l, 0, i, h, k, before)
        for _, peer in tp_near:
            for h in range(2):
                block = xg.at[l + 1, i, h * half + place]
                send(block, block, "xg", xr.at[l + 1, i, 0], {"tp": peer})
        if l + 1 == last:
            send(xg.at[l + 1, i, t, 1], res.at[i], "res", res_r.at[i], {"dp": mate})

    def expand_mate(l, i):
        arrived(rq.at[l, i], rq_r.at[l, i])
        arrived(zr.at[l, 1, i], z_r.at[l, 1, i])
        for h in range(2):
            for k in range(2):
                xq[l, i, h, k] = whole(l, 1, i, h, k, rq[l, i, h, k])
        for h in range(2):
            block, dst = xq.at[l, i, h], xg.at[l + 1, i, h * half + place]
            for _, peer in tp_near:
                send(block, dst, "xq", xr.at[l + 1, i, 0], {"tp": peer, "dp": mate})
            send(block, dst, "xq", xr.at[l + 1, i, 0], {"dp": mate})

    def finish(k, i):
        if k == 0:
            total = mx[last, i, t, 0].astype(jnp.float32)
            total = total + xg[last, i, t, 0].reshape(full, own).astype(jnp.float32)
            held = fo
        else:


            @pl.when(core == 0)
            def _():
                arrived(res.at[i], res_r.at[i])

            @pl.when(core == 1)
            def _():
                res[i] = xq[last - 1, i, t // half, 1]

            total = res[i].reshape(full, own).astype(jnp.float32)
            held = fm
        arrived(held.at[i], f_r.at[k, i])
        for j in range(held.shape[1]):
            total = total + held[i, j].astype(jnp.float32)
        mix_o[k, i] = total.astype(jnp.bfloat16).reshape(nd, r, own)

    for i in range(groups):
        loaded(xg.at[0, i, t, 0], c_own[i])
    loaded(xm, c_mate)
    pl.semaphore_wait(barrier, 2 * (nt - 1) + 3)
    def send_own(i):
        block = xg.at[0, i, t, 0]
        for n, peer in tp_peers:
            send(block, block, "xo", xr.at[0, i, 2 * n // nt], {"tp": peer})

    def send_mate(i):
        for n, peer in tp_peers:
            sem = xr.at[0, i, 2 * n // nt]
            send(xm.at[i], xg.at[0, i, t, 1], "xm", sem, {"tp": peer, "dp": mate})
        send(xm.at[i], xg.at[0, i, t, 1], "xm", xr.at[0, i, 0], {"dp": mate})

    for kind, calls in enumerate(((send_own, send_mate), (send_mate, send_own))):

        @pl.when(core == kind)
        def _():
            for i in range(groups):
                for call in calls:
                    call(i)

    loaded(gain_v.at[0], c_gain)
    send(gain_v.at[0], gain_v.at[1], "gain", gain_r.at[0], {"dp": mate})
    send_weights(0)
    for ref, sem in c_first:
        loaded(ref, sem)
    spread_gain(0)
    prepare()
    send_history(0)
    send_out(0)
    for l in range(layers):
        if l == 0:
            for i in range(groups):
                project_near(l, i)
        for i in range(groups):
            if l > 0:
                project_all(l, i)
            else:
                project_far(l, i)
        if l + 1 < layers:
            send_weights(l + 1)
        for i in range(groups):
            readout = recur(l, i)
            mix(l, i, readout)
        if l + 1 < layers:
            send_history(l + 1)
            send_out(l + 1)


            @pl.when(core == 1)
            def _():
                collect(l, 0)
                collect_mate(l, 0)
                for i in range(1, groups):
                    collect(l, i)
                    expand(l, i - 1)
                    collect_mate(l, i)
                    expand_mate(l, i - 1)
                expand(l, groups - 1)
                expand_mate(l, groups - 1)

    for i in range(groups):
        finish(0, i)
        finish(1, i)
    arrived(state_m, st_r.at[0])
    arrived(branch_m, br_r.at[0])
    all_sent("xo", xg.at[0, :, pl.ds(0, nt - 1), 0])
    all_sent("xm", xg.at[0, :, :, 1])
    all_sent("gain", gain_v.at[1])
    all_sent("wp", wp_v.at[:, 1])
    all_sent("wo", wo_v.at[:, 1])
    all_sent("aux", aux.at[:, pl.ds(0, nd - 1)])
    all_sent("px", px)

    @pl.when(core == 1)
    def _():
        all_sent("ms", ms)
        all_sent("zs", zr)
        all_sent("xg", xg.at[pl.ds(1, last), :, pl.ds(0, 2 * half - 2)])
        all_sent("xq", xg.at[pl.ds(1, last)])
        all_sent("res", res)

    @pl.when(core == 0)
    def _():
        all_sent("mq", mq)
        all_sent("rq", rq)

    all_sent("fo", fo)
    all_sent("fm", fm)
    all_sent("state", state_m)
    all_sent("branch", branch_m)


def flipped(index, mask, count):
    for bit in range(count.bit_length() - 1):
        if mask >> bit & 1:
            index = index + (1 << bit) * (1 - 2 * (index // (1 << bit) % 2))
    return index


def tail_kernel(
    mixed, state, state_m, hist, branch, branch_m, mixed_out, state_out, window_out, sem
):
    d = lax.axis_index("dp")
    core = lax.rem(d, 2)
    layers, depth = window_out.shape[:2]
    groups, r = mixed.shape[1], mixed.shape[3]

    def span(k, i):
        side = core if k == 0 else 1 - core
        return pl.ds(pl.multiple_of((side * groups + i) * r, r), r)

    pairs = []
    for i in range(groups):
        for k in range(2):
            pairs.append((mixed.at[k, i], mixed_out.at[:, span(k, i), :]))
    for l in range(layers):
        pairs.append((hist.at[l], window_out.at[l, pl.ds(0, depth - 1)]))
        for i in range(groups):
            pairs.append((state.at[l, i, d], state_out.at[l, span(0, i), :]))
            pairs.append((state_m.at[l, i], state_out.at[l, span(1, i), :]))
            pairs.append((branch.at[l, i, d], window_out.at[l, depth - 1, span(0, i), :]))
            pairs.append((branch_m.at[l, i], window_out.at[l, depth - 1, span(1, i), :]))
    stores = [pltpu.make_async_copy(src, dst, sem.at[k]) for k, (src, dst) in enumerate(pairs)]
    for copy in stores:
        copy.start()
    for copy in stores:
        copy.wait()


def fused(
    nt,
    nd,
    groups,
    stream,
    lengths,
    prior_state,
    prior_window,
    norm_gain,
    w_branch,
    w_gate_branch,
    conv_taps,
    w_in_gate,
    w_rec_gate,
    decay_param,
    w_out,
):
    layers, width, cols = w_branch.shape
    batch, own = stream.shape
    rows = batch // nd
    r = rows // (2 * groups)
    full = nd * r
    depth = prior_window.shape[2]
    window = prior_window.transpose(0, 2, 1, 3)
    bf16, f32 = jnp.bfloat16, jnp.float32
    anywhere = pl.BlockSpec(memory_space=pl.ANY)
    held = pl.BlockSpec(memory_space=pltpu.VMEM)
    dma = pltpu.SemaphoreType.DMA
    finals = pl.pallas_call(
        functools.partial(fused_kernel, nt, nd, groups),
        out_shape=(
            pltpu.VMEM((2, groups, nd, r, own), bf16),
            pltpu.VMEM((layers, groups, nd, r, cols), f32),
            pltpu.VMEM((layers, groups, r, cols), f32),
            pltpu.VMEM((layers, depth - 1, rows, cols), bf16),
            pltpu.VMEM((layers, groups, nd, r, cols), bf16),
            pltpu.VMEM((layers, groups, r, cols), bf16),
        ),
        in_specs=[pl.BlockSpec(memory_space=pltpu.HBM)] * 12,
        out_specs=(held,) * 6,
        scratch_shapes=[
            pltpu.VMEM((layers, groups, nt, 2, nd, r, own), bf16),
            pltpu.VMEM((groups, nd, r, own), bf16),
            pltpu.VMEM((layers, groups, full, 2 * cols + 128), bf16),
            pltpu.VMEM((layers, groups, full, 2 * cols + 128), bf16),
            pltpu.VMEM((layers, groups, nt, 2, full, own), bf16),
            pltpu.VMEM((layers - 1, groups, nt // 2 - 1, 2, 2, full, own), bf16),
            pltpu.VMEM((groups, nt - 1, full, own), bf16),
            pltpu.VMEM((groups, nt, full, own), bf16),
            pltpu.VMEM((groups, nd, r, own), bf16),
            pltpu.VMEM((layers - 1, groups, nt // 2, 2, 2, full, own), bf16),
            pltpu.VMEM((layers - 1, groups, 2, 2, nd, r, own), bf16),
            pltpu.VMEM((layers - 1, groups, 2, 2, nd, r, own), bf16),
            pltpu.VMEM((layers - 1, 2, groups, 2, 2, full, own), bf16),
            pltpu.VMEM((layers - 1, 2, groups, 2, 2, full, own), bf16),
            pltpu.VMEM((layers, 2, groups, 2, r, cols), f32),
            pltpu.VMEM((layers, nd, groups, 2, r, cols), f32),
            pltpu.VMEM((1, rows), jnp.int32),
            pltpu.VMEM(prior_state.shape, f32),
            pltpu.VMEM(window.shape, bf16),
            pltpu.VMEM((2,) + norm_gain.shape, f32),
            pltpu.VMEM((layers, 2, 2, width, cols), bf16),
            pltpu.VMEM(conv_taps.shape, bf16),
            pltpu.VMEM((2, layers, BLOCK, cols), bf16),
            pltpu.VMEM(decay_param.shape, f32),
            pltpu.VMEM((layers, 2, cols, width), bf16),
            pltpu.VMEM((2, layers, nt, 1, own), f32),
            pltpu.VMEM((groups, 2, full, cols), f32),
            pltpu.VMEM((groups, full, own), f32),
            dma((8 + groups + 2 * layers,)),
            dma((18,)),
            dma((layers, groups, 2)),
            dma((layers, groups, 2)),
            dma((layers - 1, groups)),
            dma((2, groups)),
            dma((groups,)),
            dma((layers - 1, groups)),
            dma((layers - 1, groups)),
            dma((layers - 1, 2, groups)),
            dma((layers,)),
            dma((layers,)),
            dma((layers,)),
            dma((1,)),
            dma((1,)),
            dma((1,)),
        ],
        compiler_params=pltpu.CompilerParams(
            collective_id=0, has_side_effects=True, vmem_limit_bytes=MAIN_VMEM
        ),
    )(
        stream.reshape(nd, rows, own),
        lengths.reshape(1, rows),
        prior_state,
        window,
        norm_gain,
        w_branch,
        w_gate_branch,
        conv_taps,
        w_in_gate,
        w_rec_gate,
        decay_param,
        w_out,
    )
    mixed, state, new_window = pl.pallas_call(
        tail_kernel,
        out_shape=(
            jax.ShapeDtypeStruct((nd, rows, own), bf16),
            jax.ShapeDtypeStruct(prior_state.shape, f32),
            jax.ShapeDtypeStruct(window.shape, bf16),
        ),
        in_specs=[held] * 6,
        out_specs=(anywhere,) * 3,
        scratch_shapes=[dma((2 * groups + layers * (1 + 4 * groups),))],
        compiler_params=pltpu.CompilerParams(vmem_limit_bytes=TAIL_VMEM),
    )(*finals)
    return mixed.reshape(batch, own), state, new_window.transpose(0, 2, 1, 3)


def step(nt, nd, *arrays):
    stream, w_branch = arrays[0], arrays[5]
    rows, cols = stream.shape[0] // nd, w_branch.shape[2]
    layers = w_branch.shape[0]
    if nd == 4 and layers > 1 and nt & (nt - 1) == 0 and cols % BLOCK == 0 and stream.shape[1] % 128 == 0 and rows % (16 * GROUPS) == 0:
        return fused(nt, nd, GROUPS, *arrays)
    return body(*arrays)


def solution(mesh):
    placed = (
        P(None, ("dp", "tp")),
        P("dp"),
        P(None, "dp", "tp"),
        P(None, "dp", None, "tp"),
        P(None, "dp"),
        P(None, "dp", "tp"),
        P(None, "dp", "tp"),
        P(None, None, "tp"),
        P(None, None, "tp"),
        P(None, None, "tp"),
        P(None, "tp"),
        P(None, "tp", "dp"),
    )
    return jax.shard_map(
        functools.partial(step, mesh.shape["tp"], mesh.shape["dp"]),
        mesh=mesh,
        in_specs=placed,
        out_specs=(P(None, ("dp", "tp")), P(None, "dp", "tp"), P(None, "dp", None, "tp")),
        check_vma=False,
    )
```

```python
import functools

import jax
import jax.numpy as jnp
from jax import lax
from jax.experimental import pallas as pl
from jax.experimental.pallas import tpu as pltpu
from jax.sharding import PartitionSpec as P

D = 4096
BLOCK = 256


epsilon = 1e-06


def from_partner(block, axis, apart):
    count = lax.axis_size(axis)
    route = []
    for low in range(count):
        high = low | 1 << apart
        if high != low and high < count:
            route += [(low, high), (high, low)]
    return lax.ppermute(block, axis, route)


def norm_rows(block_rows, gain_values, squares):
    scaling = lax.rsqrt(squares / D + epsilon)
    return (block_rows.astype(jnp.float32) * scaling * gain_values).astype(jnp.bfloat16)


def normed_input(stream_local, gain_block):
    own_width = stream_local.shape[1]
    offset = lax.axis_index("tp") * own_width
    widened = stream_local.astype(jnp.float32)
    squares = lax.psum(jnp.sum(widened * widened, axis=1, keepdims=True), ("tp", "dp"))
    own_gain = lax.dynamic_slice_in_dim(gain_block, offset, own_width, 0)
    result = lax.all_gather(norm_rows(stream_local, own_gain, squares), "tp", axis=1, tiled=True)
    return result


def peer_block(convolved):
    col_count = convolved.shape[1]
    group_size = max(BLOCK // col_count, 1)
    device = lax.axis_index("tp")
    grouped = convolved
    for bit_number in range(group_size.bit_length() - 1):
        partner = from_partner(grouped, "tp", bit_number)
        is_upper = device // (1 << bit_number) % 2 == 1
        grouped = jnp.where(
            is_upper,
            jnp.concatenate([partner, grouped], axis=1),
            jnp.concatenate([grouped, partner], axis=1),
        )
    return grouped


def block_gates(grouped, weight):
    row_count = grouped.shape[0]
    col_count = weight.shape[1]
    blocks = max(col_count // BLOCK, 1)
    block_cols = min(col_count, BLOCK)
    inputs = grouped.reshape(row_count, blocks, BLOCK)
    tables = weight.reshape(BLOCK, blocks, block_cols)
    mapped = jnp.einsum("rnk,knc->rnc", inputs, tables, preferred_element_type=jnp.float32)
    return mapped.reshape(row_count, col_count)


def recurrent_step(
    normed,
    lengths,
    prior_state,
    prior_window,
    w_branch,
    w_gate_branch,
    conv_taps,
    w_in_gate,
    w_rec_gate,
    decay_param,
    w_out,
    stream_local,
):
    col_count = w_branch.shape[1]
    summed = lax.psum_scatter(
        jnp.concatenate(
            [
                jnp.dot(normed, w_branch, preferred_element_type=jnp.float32),
                jnp.dot(normed, w_gate_branch, preferred_element_type=jnp.float32),
            ],
            axis=1,
        ).astype(jnp.bfloat16),
        "dp",
        scatter_dimension=0,
        tiled=True,
    ).astype(jnp.float32)
    branch = summed[:, :col_count].astype(jnp.bfloat16)
    gate_in = summed[:, col_count:].astype(jnp.bfloat16)
    depth = prior_window.shape[1]
    needed = depth + 1 - jnp.arange(depth, dtype=jnp.int32)
    living = lengths[:, None, None] >= needed[None, :, None]
    history = jnp.where(living, prior_window, jnp.zeros_like(prior_window))
    window = jnp.concatenate([history, branch[:, None, :]], axis=1)
    convolved = jnp.sum(
        window.astype(jnp.float32) * conv_taps.astype(jnp.float32)[None], axis=1
    ).astype(jnp.bfloat16)
    grouped = peer_block(convolved)
    input_gate = jax.nn.sigmoid(block_gates(grouped, w_in_gate))
    recur_gate = jax.nn.sigmoid(block_gates(grouped, w_rec_gate))
    log_keep = 8.0 * recur_gate * jax.nn.log_sigmoid(decay_param)
    keeping = jnp.exp(log_keep)
    feeding = jnp.sqrt(-jnp.expm1(2.0 * log_keep))
    earlier = jnp.where(lengths[:, None] >= 2, prior_state, jnp.zeros_like(prior_state))
    state = keeping * earlier + feeding * input_gate * convolved.astype(jnp.float32)
    readout = (state * jax.nn.gelu(gate_in.astype(jnp.float32))).astype(jnp.bfloat16)
    mixed = jnp.dot(
        lax.all_gather(readout, "dp", axis=0, tiled=True), w_out, preferred_element_type=jnp.float32
    )
    own_width = stream_local.shape[1]
    offset = lax.axis_index("tp") * own_width
    own_cols = lax.dynamic_slice_in_dim(mixed, offset, own_width, 1) + stream_local.astype(
        jnp.float32
    )
    terms = lax.dynamic_update_slice_in_dim(mixed, own_cols, offset, 1)
    return (terms, state, window[:, 1:])


def body(
    stream,
    lengths,
    prior_state,
    prior_window,
    norm_gain,
    w_branch,
    w_gate_branch,
    conv_taps,
    w_in_gate,
    w_rec_gate,
    decay_param,
    w_out,
):
    normed = normed_input(stream, norm_gain[0])
    terms, state_first, window_first = recurrent_step(
        normed,
        lengths,
        prior_state[0],
        prior_window[0],
        w_branch[0],
        w_gate_branch[0],
        conv_taps[0],
        w_in_gate[0],
        w_rec_gate[0],
        decay_param[0],
        w_out[0],
        stream,
    )
    carried = lax.psum(terms, "tp").astype(jnp.bfloat16)
    widened = carried.astype(jnp.float32)
    squares = lax.psum(jnp.sum(widened * widened, axis=1, keepdims=True), "dp")
    normed = norm_rows(carried, norm_gain[1], squares)
    own_width = stream.shape[1]
    first = lax.dynamic_slice_in_dim(carried, lax.axis_index("tp") * own_width, own_width, 1)
    terms, state_second, window_second = recurrent_step(
        normed,
        lengths,
        prior_state[1],
        prior_window[1],
        w_branch[1],
        w_gate_branch[1],
        conv_taps[1],
        w_in_gate[1],
        w_rec_gate[1],
        decay_param[1],
        w_out[1],
        first,
    )
    second = lax.psum_scatter(terms, "tp", scatter_dimension=1, tiled=True).astype(jnp.bfloat16)
    return (
        second,
        jnp.stack([state_first, state_second]),
        jnp.stack([window_first, window_second]),
    )


GROUPS = 2
MAIN_VMEM = 60 * 1024 * 1024
TAIL_VMEM = 4 * 1024 * 1024
MESH = pl.DeviceIdType.MESH


def negative_expm1(z):
    series = -z * (1.0 + z / 2.0 * (1.0 + z / 3.0 * (1.0 + z / 4.0 * (1.0 + z / 5.0))))
    return jnp.where(z > -0.1, series, 1.0 - jnp.exp(z))


def fused_kernel(
    nt,
    nd,
    groups,
    stream,
    lengths,
    prior_state,
    prior_window,
    norm_gain,
    w_branch,
    w_gate_branch,
    conv_taps,
    w_in_gate,
    w_rec_gate,
    decay_param,
    w_out,
    mix_o,
    state_o,
    state_m,
    hist_o,
    branch_o,
    branch_m,
    xg,
    xm,
    part,
    px,
    mx,
    ms,
    fo,
    fm,
    res,
    mq,
    rq,
    xq,
    zs,
    zr,
    am,
    aux,
    len_v,
    state_v,
    win_v,
    gain_v,
    wp_v,
    taps_v,
    gates_v,
    decay_v,
    wo_v,
    gain_s,
    acc,
    sq,
    in_sem,
    sent,
    xr,
    px_r,
    ms_r,
    f_r,
    res_r,
    mq_r,
    rq_r,
    z_r,
    aux_r,
    wp_r,
    wo_r,
    gain_r,
    st_r,
    br_r,
):
    t = lax.axis_index("tp")
    d = lax.axis_index("dp")
    core = lax.rem(d, 2)
    mate = d + 1 - 2 * core
    across = lax.rem(d + 2, nd)
    corner = lax.rem(mate + 2, nd)
    layers = w_branch.shape[0]
    last = layers - 1
    rows, own = stream.shape[1], stream.shape[2]
    r = rows // (2 * groups)
    full = nd * r
    cols = w_branch.shape[2]
    width = w_branch.shape[1]
    depth = prior_window.shape[1]

    half = nt // 2
    place = lax.rem(t, half)
    halves_of = (pl.ds(0, 128 + cols), pl.ds(128 + cols, cols))

    barrier = pltpu.get_barrier_semaphore()
    tp_peers = [(k, flipped(t, k, nt)) for k in range(nt - 1, 0, -1)]
    opposite = flipped(t, half, nt)
    tp_near = [(k, peer) for k, peer in tp_peers if k < half]
    for _, peer in tp_peers:
        for other in (d, mate):
            pl.semaphore_signal(
                barrier, inc=1, device_id={"tp": peer, "dp": other}, device_id_type=MESH
            )
    for peer in (across, corner, mate):
        pl.semaphore_signal(barrier, inc=1, device_id={"dp": peer}, device_id_type=MESH)

    counter = [0]

    def load(*pairs):
        sem = in_sem.at[counter[0]]
        counter[0] += 1
        for src, dst in pairs:
            pltpu.make_async_copy(src, dst, sem).start()
        return sem

    def loaded(ref, sem):
        pltpu.make_async_copy(ref, ref, sem).wait()

    def span(k, i):
        side = core if k == 0 else 1 - core
        return pl.ds(pl.multiple_of((side * groups + i) * r, r), r)

    c_own = [load((stream.at[:, span(0, i), :], xg.at[0, i, t, 0])) for i in range(groups)]
    c_mate = load(*[(stream.at[:, span(1, i), :], xm.at[i]) for i in range(groups)])
    c_gain = load((norm_gain, gain_v.at[0]))
    c_first = [
        (held, load((src, held)))
        for src, held in (
            (lengths, len_v),
            (conv_taps, taps_v),
            (prior_window, win_v),
            (prior_state, state_v),
        )
    ]
    c_w, c_o = [], []
    for l in range(layers):
        c_w.append(load((w_branch.at[l], wp_v.at[l, 0, 0]), (w_gate_branch.at[l], wp_v.at[l, 0, 1])))
        c_o.append(load((w_out.at[l], wo_v.at[l, 0])))
        if l == 0:
            c_gates = load((w_in_gate, gates_v.at[0]), (w_rec_gate, gates_v.at[1]))
            c_decay = load((decay_param, decay_v))

    kinds = {}

    def remote(src, dst, ssem, rsem, where):
        return pltpu.make_async_remote_copy(
            src_ref=src,
            dst_ref=dst,
            send_sem=ssem,
            recv_sem=rsem,
            device_id=where,
            device_id_type=MESH,
        )

    def send(src, dst, kind, rsem, where):
        ssem = sent.at[kinds.setdefault(kind, len(kinds))]
        remote(src, dst, ssem, rsem, where).start()

    def arrived(ref, rsem):
        remote(ref, ref, sent.at[0], rsem, {"dp": mate}).wait_recv()

    def all_sent(kind, ref):
        sem = sent.at[kinds[kind]]
        remote(ref, ref, sem, sem, {"dp": mate}).wait_send()

    def prepare():
        length = jnp.sum(
            jnp.where(
                lax.broadcasted_iota(jnp.int32, (rows, rows), 0)
                == lax.broadcasted_iota(jnp.int32, (rows, rows), 1),
                jnp.broadcast_to(len_v[...].astype(jnp.float32), (rows, rows)),
                0.0,
            ),
            axis=1,
            keepdims=True,
        )
        for l in range(layers):
            taps = taps_v[l].astype(jnp.float32)
            before = jnp.zeros((rows, cols), jnp.float32)
            for m in range(depth):
                row = win_v[l, m].astype(jnp.float32)
                row = jnp.where(length >= depth + 1 - m, row, 0.0)
                before = before + row * taps[m : m + 1]
                if m > 0:
                    hist_o[l, m - 1] = row.astype(jnp.bfloat16)
            earlier = jnp.where(length >= 2, state_v[l], 0.0)
            for k in range(2):
                for i in range(groups):
                    piece = slice((k * groups + i) * r, (k * groups + i + 1) * r)
                    am[l, k, i, 0] = before[piece]
                    am[l, k, i, 1] = earlier[piece]
            aux[l, d] = am[l, core]

    def send_history(l):
        send(am.at[l, core], aux.at[l, d], "aux", aux_r.at[l], {"dp": across})
        send(am.at[l, 1 - core], aux.at[l, d], "aux", aux_r.at[l], {"dp": corner})
        send(am.at[l, 1 - core], aux.at[l, d], "aux", aux_r.at[l], {"dp": mate})

    def send_weights(l):
        loaded(wp_v.at[l, 0], c_w[l])
        send(wp_v.at[l, 0], wp_v.at[l, 1], "wp", wp_r.at[l], {"dp": mate})

    def send_out(l):
        loaded(wo_v.at[l, 0], c_o[l])
        send(wo_v.at[l, 0], wo_v.at[l, 1], "wo", wo_r.at[l], {"dp": mate})

    def spread_gain(k):
        for l in range(layers):
            for j in range(nt):
                gain_s[k, l, j] = gain_v[k, l : l + 1, j * own : (j + 1) * own]

    def normed(l, i, k, first, count=nt // 2):
        squares = jnp.zeros((full, own), jnp.float32)
        pieces = []
        for j in range(count):
            x = xg[l, i, first + j, k].reshape(full, own).astype(jnp.float32)
            squares = squares + x * x
            pieces.append((x * gain_s[k, l, first + j]).astype(jnp.bfloat16))
        return jnp.concatenate(pieces, axis=1), squares

    def weight(l, k, w, first):
        return wp_v[l, k, w, pl.ds(pl.multiple_of(first * own, own * nt // 2), own * nt // 2), :]

    def project_near(l, i):
        arrived(xg.at[l, i, pl.ds(0, nt - 1), 0], xr.at[l, i, 0])
        first = t // (nt // 2) * (nt // 2)
        if i == 0:
            arrived(gain_v.at[1], gain_r.at[0])
            spread_gain(1)
        squares = []
        products = [None, None]
        for k in range(2):
            x, part_squares = normed(l, i, k, first)
            squares.append(part_squares)
            if i == 0 and k == 1:
                arrived(wp_v.at[l, 1], wp_r.at[l])
            for w in range(2):
                term = jnp.dot(x, weight(l, k, w, first), preferred_element_type=jnp.float32)
                products[w] = term if k == 0 else products[w] + term
        for w in range(2):
            acc[i, w] = products[w]
        sq[i] = squares[0] + squares[1]

    def project_far(l, i):
        arrived(xg.at[l, i, pl.ds(0, nt // 2)], xr.at[l, i, 1])
        send_before(l, i)
        first = (1 - t // (nt // 2)) * (nt // 2)
        x0, squares0 = normed(l, i, 0, first)
        x1, squares1 = normed(l, i, 1, first)
        publish(l, i, sq[i] + squares0 + squares1, x0, x1, first, nt // 2)

    def project_all(l, i):
        @pl.when(core == 1)
        def _():
            arrived(xg.at[l, i, pl.ds(0, 2 * half - 2)], xr.at[l, i, 0])

        @pl.when(core == 0)
        def _():
            arrived(xg.at[l, i], xr.at[l, i, 0])

        if l < last:
            send_before(l, i)
        x0, squares0 = normed(l, i, 0, 0, nt)
        x1, squares1 = normed(l, i, 1, 0, nt)
        if i == 0:
            arrived(wp_v.at[l, 1], wp_r.at[l])
        publish(l, i, squares0 + squares1, x0, x1, 0, nt)

    def send_before(l, i):
        @pl.when(core == 0)
        def _():
            for h in range(2):
                block = xg.at[l, i, h * half + place]
                send(block, rq.at[l, i, h], "rq", rq_r.at[l, i], {"dp": mate})

    def publish(l, i, squares, x0, x1, first, count):
        total = jnp.sum(squares, axis=1, keepdims=True)
        high = total.astype(jnp.bfloat16).astype(jnp.float32)
        lane = lax.broadcasted_iota(jnp.int32, (full, 128), 1)
        part[l, i, :, :128] = jnp.where(lane < 64, high, total - high).astype(jnp.bfloat16)
        for w in range(2):
            product = None
            for k, x in enumerate((x0, x1)):
                table = wp_v[l, k, w] if count == nt else weight(l, k, w, first)
                term = jnp.dot(x, table, preferred_element_type=jnp.float32)
                product = term if product is None else product + term
            if count < nt:
                product = product + acc[i, w]
            part[l, i, :, 128 + w * cols : 128 + (w + 1) * cols] = product.astype(jnp.bfloat16)
            ready = halves_of[w]
            send(part.at[l, i, :, ready], px.at[l, i, :, ready], "px", px_r.at[l, i, w], {"dp": across})

    def recur(l, i):
        if i == 0:
            if l == 0:
                loaded(gates_v, c_gates)
                loaded(decay_v, c_decay)
            arrived(aux.at[l, pl.ds(0, nd - 1)], aux_r.at[l])
        before = aux[l, :, i, 0].reshape(full, cols)
        earlier = aux[l, :, i, 1].reshape(full, cols)
        taps = taps_v[l].astype(jnp.float32)
        raw = decay_v[l : l + 1]
        log_decay = jnp.minimum(raw, 0.0) - jnp.log1p(jnp.exp(-jnp.abs(raw)))
        first, second = halves_of
        arrived(px.at[l, i, :, first], px_r.at[l, i, 0])
        summed = part[l, i, :, first].astype(jnp.float32) + px[l, i, :, first].astype(jnp.float32)
        squares = summed[:, :1] + summed[:, 64:65]
        scaling = lax.rsqrt(squares / (width * nd) + epsilon)
        branch = (summed[:, 128:] * scaling).astype(jnp.bfloat16)
        branch_o[l, i] = branch.reshape(nd, r, cols)
        convolved = (before + branch.astype(jnp.float32) * taps[depth : depth + 1]).astype(
            jnp.bfloat16
        )
        mapped = []
        for w in range(2):
            mapped.append(
                jnp.concatenate(
                    [
                        jnp.dot(
                            convolved[:, n * BLOCK : (n + 1) * BLOCK],
                            gates_v[w, l, :, n * BLOCK : (n + 1) * BLOCK],
                            preferred_element_type=jnp.float32,
                        )
                        for n in range(cols // BLOCK)
                    ],
                    axis=1,
                )
            )
        input_gate = jax.nn.sigmoid(mapped[0])
        recur_gate = jax.nn.sigmoid(mapped[1])
        log_keep = 8.0 * recur_gate * log_decay
        feeding = jnp.sqrt(negative_expm1(2.0 * log_keep))
        state = jnp.exp(log_keep) * earlier + feeding * input_gate * convolved.astype(jnp.float32)
        state_o[l, i] = state.reshape(nd, r, cols)
        arrived(px.at[l, i, :, second], px_r.at[l, i, 1])
        summed = part[l, i, :, second].astype(jnp.float32) + px[l, i, :, second].astype(jnp.float32)
        gate_in = (summed * scaling).astype(jnp.bfloat16)
        readout = (state * jax.nn.gelu(gate_in.astype(jnp.float32))).astype(jnp.bfloat16)
        return readout

    def mix(l, i, readout):
        for k in range(2):
            if i == 0 and k == 1:
                arrived(wo_v.at[l, 1], wo_r.at[l])
            mixed = jnp.dot(readout, wo_v[l, k], preferred_element_type=jnp.float32)
            for j in range(nt):
                mx[l, i, j, k] = mixed[:, j * own : (j + 1) * own].astype(jnp.bfloat16)
            if l < last:
                continue
            for n, peer in tp_peers:
                block = mx.at[l, i, peer, k]
                if k == 0:
                    send(block, fo.at[i, n - 1], "fo", f_r.at[0, i], {"tp": peer})
                else:
                    send(block, fm.at[i, n], "fm", f_r.at[1, i], {"tp": peer, "dp": mate})
            if l == last and k == 1:
                send(mx.at[l, i, t, 1], fm.at[i, 0], "fm", f_r.at[1, i], {"dp": mate})
        if l < last:

            @pl.when(core == 1)
            def _():
                for n, peer in tp_near:
                    for h in range(2):
                        block = mx.at[l, i, h * half + lax.rem(peer, half)]
                        send(block, ms.at[l, i, n - 1, h], "ms", ms_r.at[l, i], {"tp": peer})

            @pl.when(core == 0)
            def _():
                for n, peer in tp_near:
                    for h in range(2):
                        block = mx.at[l, i, h * half + lax.rem(peer, half)]
                        where = {"tp": peer, "dp": mate}
                        send(block, mq.at[l, i, n, h], "mq", mq_r.at[l, i], where)
                for h in range(2):
                    block = mx.at[l, i, h * half + place]
                    send(block, mq.at[l, i, 0, h], "mq", mq_r.at[l, i], {"dp": mate})

        send(state_o.at[l, i, mate], state_m.at[l, i], "state", st_r.at[0], {"dp": mate})
        send(branch_o.at[l, i, mate], branch_m.at[l, i], "branch", br_r.at[0], {"dp": mate})

    def collect(l, i):
        arrived(ms.at[l, i], ms_r.at[l, i])
        for h in range(2):
            for k in range(2):
                total = mx[l, i, h * half + place, k].astype(jnp.float32)
                for j in range(half - 1):
                    total = total + ms[l, i, j, h, k].astype(jnp.float32)
                zs[l, 0, i, h, k] = total.astype(jnp.bfloat16)
        send(zs.at[l, 0, i], zr.at[l, 0, i], "zs", z_r.at[l, 0, i], {"tp": opposite})

    def collect_mate(l, i):
        arrived(mq.at[l, i], mq_r.at[l, i])
        for h in range(2):
            for k in range(2):
                total = mq[l, i, 0, h, k].astype(jnp.float32)
                for j in range(1, half):
                    total = total + mq[l, i, j, h, k].astype(jnp.float32)
                zs[l, 1, i, h, k] = total.astype(jnp.bfloat16)
        send(zs.at[l, 1, i], zr.at[l, 1, i], "zs", z_r.at[l, 1, i], {"tp": opposite})

    def whole(l, which, i, h, k, before):
        total = zs[l, which, i, h, k].astype(jnp.float32) + zr[l, which, i, h, k].astype(jnp.float32)
        total = total + before.reshape(full, own).astype(jnp.float32)
        return total.astype(jnp.bfloat16).reshape(nd, r, own)

    def expand(l, i):
        arrived(zr.at[l, 0, i], z_r.at[l, 0, i])
        for h in range(2):
            for k in range(2):
                before = xg[l, i, h * half + place, k]
                xg[l + 1, i, h * half + place, k] = whole(l, 0, i, h, k, before)
        for _, peer in tp_near:
            for h in range(2):
                block = xg.at[l + 1, i, h * half + place]
                send(block, block, "xg", xr.at[l + 1, i, 0], {"tp": peer})
        if l + 1 == last:
            send(xg.at[l + 1, i, t, 1], res.at[i], "res", res_r.at[i], {"dp": mate})

    def expand_mate(l, i):
        arrived(rq.at[l, i], rq_r.at[l, i])
        arrived(zr.at[l, 1, i], z_r.at[l, 1, i])
        for h in range(2):
            for k in range(2):
                xq[l, i, h, k] = whole(l, 1, i, h, k, rq[l, i, h, k])
        for where in [{"tp": peer, "dp": mate} for _, peer in tp_near] + [{"dp": mate}]:
            for h in range(2):
                block, dst = xq.at[l, i, h], xg.at[l + 1, i, h * half + place]
                send(block, dst, "xq", xr.at[l + 1, i, 0], where)

    def finish(k, i):
        if k == 0:
            total = mx[last, i, t, 0].astype(jnp.float32)
            total = total + xg[last, i, t, 0].reshape(full, own).astype(jnp.float32)
            held = fo
        else:


            @pl.when(core == 0)
            def _():
                arrived(res.at[i], res_r.at[i])

            @pl.when(core == 1)
            def _():
                res[i] = xq[last - 1, i, t // half, 1]

            total = res[i].reshape(full, own).astype(jnp.float32)
            held = fm
        arrived(held.at[i], f_r.at[k, i])
        for j in range(held.shape[1]):
            total = total + held[i, j].astype(jnp.float32)
        mix_o[k, i] = total.astype(jnp.bfloat16).reshape(nd, r, own)

    for i in range(groups):
        loaded(xg.at[0, i, t, 0], c_own[i])
    loaded(xm, c_mate)
    pl.semaphore_wait(barrier, 2 * (nt - 1) + 3)
    def send_own(i):
        block = xg.at[0, i, t, 0]
        for n, peer in tp_peers:
            send(block, block, "xo", xr.at[0, i, 2 * n // nt], {"tp": peer})

    def send_mate(i):
        for n, peer in tp_peers:
            sem = xr.at[0, i, 2 * n // nt]
            send(xm.at[i], xg.at[0, i, t, 1], "xm", sem, {"tp": peer, "dp": mate})
        send(xm.at[i], xg.at[0, i, t, 1], "xm", xr.at[0, i, 0], {"dp": mate})

    for kind, calls in enumerate(((send_own, send_mate), (send_mate, send_own))):

        @pl.when(core == kind)
        def _():
            for i in range(groups):
                for call in calls:
                    call(i)

    loaded(gain_v.at[0], c_gain)
    send(gain_v.at[0], gain_v.at[1], "gain", gain_r.at[0], {"dp": mate})
    send_weights(0)
    for ref, sem in c_first:
        loaded(ref, sem)
    spread_gain(0)
    prepare()
    send_history(0)
    send_out(0)
    for l in range(layers):
        if l == 0:
            for i in range(groups):
                project_near(l, i)
        for i in range(groups):
            if l > 0:
                project_all(l, i)
            else:
                project_far(l, i)
        if l + 1 < layers:
            send_weights(l + 1)
        for i in range(groups):
            readout = recur(l, i)
            mix(l, i, readout)
        if l + 1 < layers:
            send_history(l + 1)
            send_out(l + 1)


            @pl.when(core == 1)
            def _():
                collect(l, 0)
                collect_mate(l, 0)
                for i in range(1, groups):
                    collect(l, i)
                    expand(l, i - 1)
                    collect_mate(l, i)
                    expand_mate(l, i - 1)
                expand(l, groups - 1)
                expand_mate(l, groups - 1)

    for i in range(groups):
        finish(0, i)
        finish(1, i)
    arrived(state_m, st_r.at[0])
    arrived(branch_m, br_r.at[0])
    all_sent("xo", xg.at[0, :, pl.ds(0, nt - 1), 0])
    all_sent("xm", xg.at[0, :, :, 1])
    all_sent("gain", gain_v.at[1])
    all_sent("wp", wp_v.at[:, 1])
    all_sent("wo", wo_v.at[:, 1])
    all_sent("aux", aux.at[:, pl.ds(0, nd - 1)])
    all_sent("px", px)

    @pl.when(core == 1)
    def _():
        all_sent("ms", ms)
        all_sent("zs", zr)
        all_sent("xg", xg.at[pl.ds(1, last), :, pl.ds(0, 2 * half - 2)])
        all_sent("xq", xg.at[pl.ds(1, last)])
        all_sent("res", res)

    @pl.when(core == 0)
    def _():
        all_sent("mq", mq)
        all_sent("rq", rq)

    all_sent("fo", fo)
    all_sent("fm", fm)
    all_sent("state", state_m)
    all_sent("branch", branch_m)


def flipped(index, mask, count):
    for bit in range(count.bit_length() - 1):
        if mask >> bit & 1:
            index = index + (1 << bit) * (1 - 2 * (index // (1 << bit) % 2))
    return index


def tail_kernel(
    mixed, state, state_m, hist, branch, branch_m, mixed_out, state_out, window_out, sem
):
    d = lax.axis_index("dp")
    core = lax.rem(d, 2)
    layers, depth = window_out.shape[:2]
    groups, r = mixed.shape[1], mixed.shape[3]

    def span(k, i):
        side = core if k == 0 else 1 - core
        return pl.ds(pl.multiple_of((side * groups + i) * r, r), r)

    pairs = []
    for i in range(groups):
        for k in range(2):
            pairs.append((mixed.at[k, i], mixed_out.at[:, span(k, i), :]))
    for l in range(layers):
        pairs.append((hist.at[l], window_out.at[l, pl.ds(0, depth - 1)]))
        for i in range(groups):
            pairs.append((state.at[l, i, d], state_out.at[l, span(0, i), :]))
            pairs.append((state_m.at[l, i], state_out.at[l, span(1, i), :]))
            pairs.append((branch.at[l, i, d], window_out.at[l, depth - 1, span(0, i), :]))
            pairs.append((branch_m.at[l, i], window_out.at[l, depth - 1, span(1, i), :]))
    stores = [pltpu.make_async_copy(src, dst, sem.at[k]) for k, (src, dst) in enumerate(pairs)]
    for copy in stores:
        copy.start()
    for copy in stores:
        copy.wait()


def fused(
    nt,
    nd,
    groups,
    stream,
    lengths,
    prior_state,
    prior_window,
    norm_gain,
    w_branch,
    w_gate_branch,
    conv_taps,
    w_in_gate,
    w_rec_gate,
    decay_param,
    w_out,
):
    layers, width, cols = w_branch.shape
    batch, own = stream.shape
    rows = batch // nd
    r = rows // (2 * groups)
    full = nd * r
    depth = prior_window.shape[2]
    window = prior_window.transpose(0, 2, 1, 3)
    bf16, f32 = jnp.bfloat16, jnp.float32
    anywhere = pl.BlockSpec(memory_space=pl.ANY)
    held = pl.BlockSpec(memory_space=pltpu.VMEM)
    dma = pltpu.SemaphoreType.DMA
    finals = pl.pallas_call(
        functools.partial(fused_kernel, nt, nd, groups),
        out_shape=(
            pltpu.VMEM((2, groups, nd, r, own), bf16),
            pltpu.VMEM((layers, groups, nd, r, cols), f32),
            pltpu.VMEM((layers, groups, r, cols), f32),
            pltpu.VMEM((layers, depth - 1, rows, cols), bf16),
            pltpu.VMEM((layers, groups, nd, r, cols), bf16),
            pltpu.VMEM((layers, groups, r, cols), bf16),
        ),
        in_specs=[pl.BlockSpec(memory_space=pltpu.HBM)] * 12,
        out_specs=(held,) * 6,
        scratch_shapes=[
            pltpu.VMEM((layers, groups, nt, 2, nd, r, own), bf16),
            pltpu.VMEM((groups, nd, r, own), bf16),
            pltpu.VMEM((layers, groups, full, 2 * cols + 128), bf16),
            pltpu.VMEM((layers, groups, full, 2 * cols + 128), bf16),
            pltpu.VMEM((layers, groups, nt, 2, full, own), bf16),
            pltpu.VMEM((layers - 1, groups, nt // 2 - 1, 2, 2, full, own), bf16),
            pltpu.VMEM((groups, nt - 1, full, own), bf16),
            pltpu.VMEM((groups, nt, full, own), bf16),
            pltpu.VMEM((groups, nd, r, own), bf16),
            pltpu.VMEM((layers - 1, groups, nt // 2, 2, 2, full, own), bf16),
            pltpu.VMEM((layers - 1, groups, 2, 2, nd, r, own), bf16),
            pltpu.VMEM((layers - 1, groups, 2, 2, nd, r, own), bf16),
            pltpu.VMEM((layers - 1, 2, groups, 2, 2, full, own), bf16),
            pltpu.VMEM((layers - 1, 2, groups, 2, 2, full, own), bf16),
            pltpu.VMEM((layers, 2, groups, 2, r, cols), f32),
            pltpu.VMEM((layers, nd, groups, 2, r, cols), f32),
            pltpu.VMEM((1, rows), jnp.int32),
            pltpu.VMEM(prior_state.shape, f32),
            pltpu.VMEM(window.shape, bf16),
            pltpu.VMEM((2,) + norm_gain.shape, f32),
            pltpu.VMEM((layers, 2, 2, width, cols), bf16),
            pltpu.VMEM(conv_taps.shape, bf16),
            pltpu.VMEM((2, layers, BLOCK, cols), bf16),
            pltpu.VMEM(decay_param.shape, f32),
            pltpu.VMEM((layers, 2, cols, width), bf16),
            pltpu.VMEM((2, layers, nt, 1, own), f32),
            pltpu.VMEM((groups, 2, full, cols), f32),
            pltpu.VMEM((groups, full, own), f32),
            dma((8 + groups + 2 * layers,)),
            dma((18,)),
            dma((layers, groups, 2)),
            dma((layers, groups, 2)),
            dma((layers - 1, groups)),
            dma((2, groups)),
            dma((groups,)),
            dma((layers - 1, groups)),
            dma((layers - 1, groups)),
            dma((layers - 1, 2, groups)),
            dma((layers,)),
            dma((layers,)),
            dma((layers,)),
            dma((1,)),
            dma((1,)),
            dma((1,)),
        ],
        compiler_params=pltpu.CompilerParams(
            collective_id=0, has_side_effects=True, vmem_limit_bytes=MAIN_VMEM
        ),
    )(
        stream.reshape(nd, rows, own),
        lengths.reshape(1, rows),
        prior_state,
        window,
        norm_gain,
        w_branch,
        w_gate_branch,
        conv_taps,
        w_in_gate,
        w_rec_gate,
        decay_param,
        w_out,
    )
    mixed, state, new_window = pl.pallas_call(
        tail_kernel,
        out_shape=(
            jax.ShapeDtypeStruct((nd, rows, own), bf16),
            jax.ShapeDtypeStruct(prior_state.shape, f32),
            jax.ShapeDtypeStruct(window.shape, bf16),
        ),
        in_specs=[held] * 6,
        out_specs=(anywhere,) * 3,
        scratch_shapes=[dma((2 * groups + layers * (1 + 4 * groups),))],
        compiler_params=pltpu.CompilerParams(vmem_limit_bytes=TAIL_VMEM),
    )(*finals)
    return mixed.reshape(batch, own), state, new_window.transpose(0, 2, 1, 3)


def step(nt, nd, *arrays):
    stream, w_branch = arrays[0], arrays[5]
    rows, cols = stream.shape[0] // nd, w_branch.shape[2]
    layers = w_branch.shape[0]
    if nd == 4 and layers > 1 and nt & (nt - 1) == 0 and cols % BLOCK == 0 and stream.shape[1] % 128 == 0 and rows % (16 * GROUPS) == 0:
        return fused(nt, nd, GROUPS, *arrays)
    return body(*arrays)


def solution(mesh):
    placed = (
        P(None, ("dp", "tp")),
        P("dp"),
        P(None, "dp", "tp"),
        P(None, "dp", None, "tp"),
        P(None, "dp"),
        P(None, "dp", "tp"),
        P(None, "dp", "tp"),
        P(None, None, "tp"),
        P(None, None, "tp"),
        P(None, None, "tp"),
        P(None, "tp"),
        P(None, "tp", "dp"),
    )
    return jax.shard_map(
        functools.partial(step, mesh.shape["tp"], mesh.shape["dp"]),
        mesh=mesh,
        in_specs=placed,
        out_specs=(P(None, ("dp", "tp")), P(None, "dp", "tp"), P(None, "dp", None, "tp")),
        check_vma=False,
    )
```
